512 devices in a mesh: sp: 32 (over z, core), tp: 16 (over y, x).
Axes of the slice: x: 4, y: 4, z: 16, core: 2. Of those that a mesh axis runs over, the one named last changes fastest.
Arguments:
- target: bfloat16 [4096, 2048], P(('sp', 'tp')), may hold values from -3 to 3
- source: bfloat16 [24576, 2048], P(('sp', 'tp')), may hold values from -6 to 6
- target_gain: float32 [2048], replicated, may hold values from 0.1 to 1.9
- source_gain: float32 [2048], replicated, may hold values from 0.1 to 1.9
- query_weight: bfloat16 [2048, 2048], P(None, 'tp'), may hold values from -0.125 to 0.125
- key_matrix: bfloat16 [2048, 256], replicated, may hold values from -0.125 to 0.125
- value_matrix: bfloat16 [2048, 256], replicated, may hold values from -0.125 to 0.125
- query_gain: float32 [16, 128], P('tp'), may hold values from 0.24 to 20
- key_gain: float32 [2, 128], replicated, may hold values from 1.2 to 4
- out_weight: bfloat16 [2048, 2048], P('tp'), may hold values from -0.125 to 0.125
Outputs:
- updated_target: bfloat16 [4096, 2048], P(('sp', 'tp'))
The draws below stay inside these ranges and needn't reach their ends.
All inputs are finite; a program needn't handle non-finite values.
Results may differ from the reference program's by a relative error of at most 0.018.
The reference program's roundings to bfloat16 on the way count: a program that leaves them out, or rounds other values in their place, can miss the bound.
Values may be sent and summed in bfloat16 or wider, within the bound.
No kernel may reach another device: no remote copies, remote signals or barrier semaphores. Data moves between devices by JAX's collectives and lax.ppermute only.
A program may use at most 64 MiB of HBM per device.

```python
import math
import jax
import jax.numpy as jnp
from jax import lax

MODEL_WIDTH = 2048
QUERY_HEAD_COUNT = 16
KEY_VALUE_HEADS = 2
HEAD_SIZE = 128
TARGET_PER_SHARD = 128
TGT = 4096
SOURCE_LENGTH = 24576
N_SP = 32


def draw_query_gain(key, part):
    random_cell_key = jax.random.fold_in(jax.random.fold_in(key, 17), 1)
    return jnp.exp(jax.random.uniform(random_cell_key, (QUERY_HEAD_COUNT, HEAD_SIZE), jnp.float32, math.log(1.2), math.log(2.2)))


def draw_key_gain(key, part):
    random_cell_key = jax.random.fold_in(key, 29)
    return jnp.exp(jax.random.uniform(random_cell_key, (KEY_VALUE_HEADS, HEAD_SIZE), jnp.float32, math.log(1.2), math.log(2.2)))


def steps_of(rng, shape, shards, low, largest):
    def one(axis_at, parts):
        steps = jax.random.uniform(jax.random.fold_in(jax.random.fold_in(rng, 6), axis_at), (parts,), jnp.float32, low / len(shards), largest / len(shards))
        return jnp.repeat(jnp.exp(steps), shape[axis_at] // parts).reshape((-1,) + (1,) * (len(shape) - axis_at - 1))

    level = one(*shards[0])
    for cut in shards[1:]:
        level = level * one(*cut)
    return level


def centred(own_key, extent, width, reach, cuts=(), kind=jnp.bfloat16):
    entries = width * jax.random.normal(own_key, extent, jnp.float32)
    if cuts:
        entries = entries * steps_of(own_key, extent, cuts, -0.22, 0.18)
    return jnp.clip(entries, -reach, reach).astype(kind)


def setup_inputs(seed: int = 0) -> dict:
    seeds = jax.random.split(jax.random.key(seed), 11)
    target = centred(seeds[0], (TGT, MODEL_WIDTH), 0.5, 3.0, ((0, 512),))
    source = centred(seeds[1], (SOURCE_LENGTH, MODEL_WIDTH), 1.0, 6.0, ((0, 512),))
    target_gain = jnp.clip(1.0 + 0.18 * jax.random.normal(seeds[2], (MODEL_WIDTH,), jnp.float32), 0.1, 1.9)
    source_gain = jnp.clip(1.0 + 0.18 * jax.random.normal(seeds[3], (MODEL_WIDTH,), jnp.float32), 0.1, 1.9)
    query_weight = centred(seeds[4], (MODEL_WIDTH, QUERY_HEAD_COUNT * HEAD_SIZE), MODEL_WIDTH ** -0.5, 0.125, ((1, 16),))
    key_matrix = centred(seeds[5], (MODEL_WIDTH, KEY_VALUE_HEADS * HEAD_SIZE), MODEL_WIDTH ** -0.5, 0.125)
    value_matrix = centred(seeds[6], (MODEL_WIDTH, KEY_VALUE_HEADS * HEAD_SIZE), MODEL_WIDTH ** -0.5, 0.125)
    query_gain = draw_query_gain(jax.random.fold_in(seeds[10], 71), 0)
    key_gain = draw_key_gain(jax.random.fold_in(seeds[10], 71), 0)
    out_weight = centred(seeds[9], (QUERY_HEAD_COUNT * HEAD_SIZE, MODEL_WIDTH), (QUERY_HEAD_COUNT * HEAD_SIZE) ** -0.5, 0.125, ((0, 16),))
    return dict(target=target, source=source, target_gain=target_gain, source_gain=source_gain, query_weight=query_weight, key_matrix=key_matrix, value_matrix=value_matrix, query_gain=query_gain, key_gain=key_gain, out_weight=out_weight)


EPSILON = 1e-06

def normed(values_in, gain):
    return values_in * lax.rsqrt(lax.optimization_barrier(jnp.mean(values_in * values_in, axis=-1, keepdims=True)) + EPSILON) * gain

def reference(target, source, target_gain, source_gain, query_weight, key_matrix, value_matrix, query_gain, key_gain, out_weight):
    normed_source_rows = normed(source.astype(jnp.float32), source_gain).astype(jnp.bfloat16)
    unnormed_keys = jnp.dot(normed_source_rows, key_matrix, preferred_element_type=jnp.float32).reshape(SOURCE_LENGTH, KEY_VALUE_HEADS, HEAD_SIZE)
    key_rows = normed(unnormed_keys, key_gain).astype(jnp.bfloat16)
    value_vectors = jnp.dot(normed_source_rows, value_matrix, preferred_element_type=jnp.float32).astype(jnp.bfloat16).reshape(SOURCE_LENGTH, KEY_VALUE_HEADS, HEAD_SIZE)
    target_normed = normed(target.astype(jnp.float32), target_gain).astype(jnp.bfloat16)
    raw_queries = jnp.dot(target_normed, query_weight, preferred_element_type=jnp.float32).reshape(TGT, QUERY_HEAD_COUNT, HEAD_SIZE)
    query_vectors = normed(raw_queries, query_gain).astype(jnp.bfloat16)
    heads_per_group = QUERY_HEAD_COUNT // KEY_VALUE_HEADS
    query_tiles = query_vectors.reshape(N_SP, TARGET_PER_SHARD, KEY_VALUE_HEADS, heads_per_group, HEAD_SIZE)
    key_float = key_rows.astype(jnp.float32)
    value_float = value_vectors.astype(jnp.float32)
    score_scale = 1.0 / math.sqrt(HEAD_SIZE)

    def by_block(query_block):
        scores = jnp.einsum('rgqd,ngd->rgqn', query_block.astype(jnp.float32), key_float) * score_scale
        maxima = lax.optimization_barrier(jnp.max(scores, axis=-1, keepdims=True))
        weights = jnp.exp(scores - maxima)
        totals = lax.optimization_barrier(jnp.sum(weights, axis=-1))
        shares = lax.optimization_barrier(weights.astype(jnp.bfloat16)).astype(jnp.float32)
        summed = jnp.einsum('rgqn,ngd->rgqd', shares, value_float)
        return (summed / totals[..., None]).astype(jnp.bfloat16)
    attended = lax.map(by_block, query_tiles).reshape(TGT, QUERY_HEAD_COUNT * HEAD_SIZE)
    update = jnp.dot(attended, out_weight, preferred_element_type=jnp.float32)
    return (target.astype(jnp.float32) + update).astype(jnp.bfloat16)
```

```python
import math

import jax
import jax.numpy as jnp
from jax import lax
from jax.experimental import pallas as pl
from jax.experimental.pallas import tpu as pltpu
from jax.sharding import PartitionSpec as P


QUERY_HEAD_COUNT = 16
KEY_VALUE_HEADS = 2
HEAD_SIZE = 128
GROUP = QUERY_HEAD_COUNT // KEY_VALUE_HEADS
EPSILON = 1e-06
EXP2_SCALE = math.log2(math.e) / math.sqrt(HEAD_SIZE)
STAT_ROWS = 16

VMEM = pl.BlockSpec(memory_space=pltpu.VMEM)


def cost(flops, nbytes, transcendentals=0):
    return pl.CostEstimate(
        flops=flops, bytes_accessed=nbytes, transcendentals=transcendentals
    )


def normed(values_in, gain):
    return (
        values_in
        * lax.rsqrt(jnp.mean(values_in * values_in, axis=-1, keepdims=True) + EPSILON)
        * gain
    )


def key_value_kernel(source, gain, key_matrix, value_matrix, key_gain, own, other):
    second = lax.axis_index("tp") >= GROUP
    rows = normed(source[...].astype(jnp.float32), gain[...]).astype(jnp.bfloat16)
    raw = jnp.dot(rows, key_matrix[...], preferred_element_type=jnp.float32)
    values = jnp.dot(rows, value_matrix[...], preferred_element_type=jnp.float32)
    values = values.astype(jnp.bfloat16)
    heads = []
    for h in range(KEY_VALUE_HEADS):
        at = slice(h * HEAD_SIZE, (h + 1) * HEAD_SIZE)
        keys = normed(raw[:, at], key_gain[h : h + 1, :]).astype(jnp.bfloat16)
        heads.append(jnp.concatenate([keys, values[:, at]], axis=1))
    own[...] = jnp.where(second, heads[1], heads[0])
    other[...] = jnp.where(second, heads[0], heads[1])


def query_kernel(target, gain, weight, head_gain, copies):
    rows = normed(target[...].astype(jnp.float32), gain[...]).astype(jnp.bfloat16)
    raw = jnp.dot(rows, weight[...], preferred_element_type=jnp.float32)
    queries = normed(raw, head_gain[...]).astype(jnp.bfloat16)
    for i in range(GROUP):
        copies[i] = queries


def in_three(x):
    first = x.astype(jnp.bfloat16)
    rest = x - first.astype(jnp.float32)
    second = rest.astype(jnp.bfloat16)
    third = (rest - second.astype(jnp.float32)).astype(jnp.bfloat16)
    return [first, second, third]


def attention_kernel(queries, near, far, out):
    per_tile = 2
    rows = per_tile * HEAD_SIZE
    at_row = lax.broadcasted_iota(jnp.int32, (HEAD_SIZE, HEAD_SIZE), 0)
    at_lane = lax.broadcasted_iota(jnp.int32, (HEAD_SIZE, HEAD_SIZE), 1)
    eye = (at_row == at_lane).astype(jnp.float32)

    def as_row(column):
        return jnp.sum(eye * column, axis=0, keepdims=True)

    for tile in range(GROUP // per_tile):
        q = queries[tile * per_tile : (tile + 1) * per_tile].reshape(rows, HEAD_SIZE)
        scores = [
            lax.dot_general(
                q,
                kv[:, :HEAD_SIZE],
                (((1,), (1,)), ((), ())),
                preferred_element_type=jnp.float32,
            )
            for kv in (near, far)
        ]
        peak = jnp.maximum(
            jnp.max(scores[0], axis=-1, keepdims=True),
            jnp.max(scores[1], axis=-1, keepdims=True),
        )
        total, weighted = 0.0, 0.0
        for kv, s in zip((near, far), scores):
            weights = jnp.exp2((s - peak) * EXP2_SCALE)
            total += jnp.sum(weights, axis=-1, keepdims=True)
            weighted += jnp.dot(
                weights.astype(jnp.bfloat16),
                kv[:, HEAD_SIZE:],
                preferred_element_type=jnp.float32,
            )
        for i in range(per_tile):
            at = slice(i * HEAD_SIZE, (i + 1) * HEAD_SIZE)
            head = tile * per_tile + i
            out[head, :HEAD_SIZE, :] = weighted[at].astype(jnp.bfloat16)
            stats = in_three(as_row(peak[at])) + in_three(as_row(total[at]))
            empty = jnp.zeros((STAT_ROWS - len(stats), HEAD_SIZE), jnp.bfloat16)
            out[head, HEAD_SIZE:, :] = jnp.concatenate(stats + [empty], axis=0)


def output_kernel(partials, weight, out):
    at_row = lax.broadcasted_iota(jnp.int32, (HEAD_SIZE, HEAD_SIZE), 0)
    at_lane = lax.broadcasted_iota(jnp.int32, (HEAD_SIZE, HEAD_SIZE), 1)
    eye = (at_row == at_lane).astype(jnp.float32)
    peaks, totals = [], []
    for j in range(GROUP):
        stats = partials[j, HEAD_SIZE:, :].astype(jnp.float32)
        peaks.append(stats[0:1] + stats[1:2] + stats[2:3])
        totals.append(stats[3:4] + stats[4:5] + stats[5:6])
    peak = peaks[0]
    for p in peaks[1:]:
        peak = jnp.maximum(peak, p)
    fades = [jnp.exp2((p - peak) * EXP2_SCALE) for p in peaks]
    total = fades[0] * totals[0]
    for f, t in zip(fades[1:], totals[1:]):
        total += f * t
    attended = 0.0
    for j in range(GROUP):
        column = jnp.sum(eye * (fades[j] / total), axis=1, keepdims=True)
        attended += column * partials[j, :HEAD_SIZE, :].astype(jnp.float32)
    update = jnp.dot(
        attended.astype(jnp.bfloat16), weight[...], preferred_element_type=jnp.float32
    )
    out[...] = update.astype(jnp.bfloat16).reshape(out.shape)


def final_kernel(target, parts, out):
    update = parts[0].astype(jnp.float32)
    for i in range(1, parts.shape[0]):
        update += parts[i].astype(jnp.float32)
    out[...] = (target[...].astype(jnp.float32) + update).astype(jnp.bfloat16)


def call(kernel, outs, estimate, count):
    return pl.pallas_call(
        kernel,
        out_shape=outs,
        in_specs=[VMEM] * count,
        out_specs=jax.tree.map(lambda _: VMEM, outs),
        cost_estimate=estimate,
        compiler_params=pltpu.CompilerParams(vmem_limit_bytes=48 * 1024 * 1024),
    )


def bf16(*shape):
    return jax.ShapeDtypeStruct(shape, jnp.bfloat16)


def body(
    target,
    source,
    target_gain,
    source_gain,
    query_weight,
    key_matrix,
    value_matrix,
    query_gain,
    key_gain,
    out_weight,
):
    width = target.shape[1]
    tp = lax.axis_size("tp")
    sp = lax.axis_size("sp")
    own_rows = target.shape[0]
    block = own_rows * tp
    source_rows = source.shape[0]
    halves = [[i + h * GROUP for i in range(GROUP)] for h in range(KEY_VALUE_HEADS)]
    along_z = [[core + 2 * z for z in range(sp // 2)] for core in range(2)]

    everyone = lax.all_to_all(
        jnp.broadcast_to(target, (tp, own_rows, width)), "tp", 0, 0, tiled=True
    ).reshape(block, width)
    own, other = call(
        key_value_kernel,
        (bf16(source_rows, 2 * HEAD_SIZE), bf16(source_rows, 2 * HEAD_SIZE)),
        cost(2 * source_rows * width * 512, 2400000),
        5,
    )(source, source_gain.reshape(1, width), key_matrix, value_matrix, key_gain)
    received = lax.ppermute(other, "tp", [(i, i ^ GROUP) for i in range(tp)])
    copies = call(
        query_kernel,
        bf16(GROUP, block, HEAD_SIZE),
        cost(2 * block * width * HEAD_SIZE, 1400000),
        4,
    )(everyone, target_gain.reshape(1, width), query_weight, query_gain)
    all_queries = lax.all_to_all(
        copies, "tp", 0, 0, tiled=True, axis_index_groups=halves
    )
    near = lax.all_gather(
        jnp.concatenate([own, received], axis=0),
        "sp",
        axis=0,
        tiled=True,
        axis_index_groups=along_z,
    )
    far = lax.ppermute(near, "sp", [(i, i ^ 1) for i in range(sp)])
    keys = 2 * near.shape[0]
    partials = call(
        attention_kernel,
        bf16(GROUP, block + STAT_ROWS, HEAD_SIZE),
        cost(4 * GROUP * block * keys * HEAD_SIZE, 2500000, GROUP * block * keys),
        3,
    )(all_queries, near, far)
    mine = lax.all_to_all(partials, "tp", 0, 0, tiled=True, axis_index_groups=halves)
    update = call(
        output_kernel,
        bf16(tp, own_rows, width),
        cost(2 * block * width * HEAD_SIZE, 1400000),
        2,
    )(mine, out_weight)
    parts = lax.all_to_all(update, "tp", 0, 0, tiled=True)
    return call(
        final_kernel, bf16(own_rows, width), cost(tp * own_rows * width, 600000), 2
    )(target, parts)


def solution(mesh):
    return jax.shard_map(
        body,
        mesh=mesh,
        in_specs=(
            P(("sp", "tp"), None),
            P(("sp", "tp"), None),
            P(),
            P(),
            P(None, "tp"),
            P(),
            P(),
            P("tp", None),
            P(),
            P("tp", None),
        ),
        out_specs=P(("sp", "tp"), None),
        check_vma=False,
    )
```

```python
import math

import jax
import jax.numpy as jnp
from jax import lax
from jax.experimental import pallas as pl
from jax.experimental.pallas import tpu as pltpu
from jax.sharding import PartitionSpec as P


QUERY_HEAD_COUNT = 16
KEY_VALUE_HEADS = 2
HEAD_SIZE = 128
GROUP = QUERY_HEAD_COUNT // KEY_VALUE_HEADS
EPSILON = 1e-06
EXP2_SCALE = math.log2(math.e) / math.sqrt(HEAD_SIZE)
STAT_ROWS = 16

VMEM = pl.BlockSpec(memory_space=pltpu.VMEM)
HBM = pl.BlockSpec(memory_space=pltpu.HBM)


def cost(flops, nbytes, transcendentals=0):
    return pl.CostEstimate(
        flops=flops, bytes_accessed=nbytes, transcendentals=transcendentals
    )


def normed(values_in, gain):
    return (
        values_in
        * lax.rsqrt(jnp.mean(values_in * values_in, axis=-1, keepdims=True) + EPSILON)
        * gain
    )


def key_value_kernel(
    source, gain, key_matrix, value_matrix, key_gain, own, other, key_part, value_part, arrived
):
    depth = key_part.shape[1]
    parts = key_part.shape[0]
    copies = [
        pltpu.make_async_copy(
            matrix.at[pl.ds(i * depth, depth), :], buffer.at[i], arrived.at[i, j]
        )
        for i in range(parts)
        for j, (matrix, buffer) in enumerate(
            ((key_matrix, key_part), (value_matrix, value_part))
        )
    ]
    for c in copies:
        c.start()
    second = lax.axis_index("tp") >= GROUP
    rows = normed(source[...].astype(jnp.float32), gain[...]).astype(jnp.bfloat16)
    raw, values = 0.0, 0.0
    for i in range(parts):
        copies[2 * i].wait()
        copies[2 * i + 1].wait()
        part = rows[:, i * depth : (i + 1) * depth]
        raw += jnp.dot(part, key_part[i], preferred_element_type=jnp.float32)
        values += jnp.dot(part, value_part[i], preferred_element_type=jnp.float32)
    values = values.astype(jnp.bfloat16)
    heads = []
    for h in range(KEY_VALUE_HEADS):
        at = slice(h * HEAD_SIZE, (h + 1) * HEAD_SIZE)
        keys = normed(raw[:, at], key_gain[h : h + 1, :]).astype(jnp.bfloat16)
        heads.append(jnp.concatenate([keys, values[:, at]], axis=1))
    own[...] = jnp.where(second, heads[1], heads[0])
    other[...] = jnp.where(second, heads[0], heads[1])


def query_kernel(target, gain, weight, head_gain, copies):
    rows = normed(target[...].astype(jnp.float32), gain[...]).astype(jnp.bfloat16)
    raw = jnp.dot(rows, weight[...], preferred_element_type=jnp.float32)
    queries = normed(raw, head_gain[...]).astype(jnp.bfloat16)
    for i in range(GROUP):
        copies[i] = queries


def in_three(x):
    first = x.astype(jnp.bfloat16)
    rest = x - first.astype(jnp.float32)
    second = rest.astype(jnp.bfloat16)
    third = (rest - second.astype(jnp.float32)).astype(jnp.bfloat16)
    return [first, second, third]


def attention_kernel(queries, near, far, out):
    per_tile = 2
    rows = per_tile * HEAD_SIZE
    at_row = lax.broadcasted_iota(jnp.int32, (HEAD_SIZE, HEAD_SIZE), 0)
    at_lane = lax.broadcasted_iota(jnp.int32, (HEAD_SIZE, HEAD_SIZE), 1)
    eye = (at_row == at_lane).astype(jnp.float32)

    def as_row(column):
        return jnp.sum(eye * column, axis=0, keepdims=True)

    for tile in range(GROUP // per_tile):
        q = queries[tile * per_tile : (tile + 1) * per_tile].reshape(rows, HEAD_SIZE)
        scores = [
            lax.dot_general(
                q,
                kv[:, :HEAD_SIZE],
                (((1,), (1,)), ((), ())),
                preferred_element_type=jnp.float32,
            )
            for kv in (near, far)
        ]
        peak = jnp.maximum(
            jnp.max(scores[0], axis=-1, keepdims=True),
            jnp.max(scores[1], axis=-1, keepdims=True),
        )
        total, weighted = 0.0, 0.0
        for kv, s in zip((near, far), scores):
            weights = jnp.exp2((s - peak) * EXP2_SCALE)
            total += jnp.sum(weights, axis=-1, keepdims=True)
            weighted += jnp.dot(
                weights.astype(jnp.bfloat16),
                kv[:, HEAD_SIZE:],
                preferred_element_type=jnp.float32,
            )
        for odd in range(2):
            def picked(column):
                return jnp.concatenate(
                    [column[i : i + 8] for i in range(8 * odd, rows, 16)], axis=0
                )

            to = tile * 2 + odd
            out[to, :HEAD_SIZE, :] = picked(weighted).astype(jnp.bfloat16)
            stats = in_three(as_row(picked(peak))) + in_three(as_row(picked(total)))
            empty = jnp.zeros((STAT_ROWS - len(stats), HEAD_SIZE), jnp.bfloat16)
            out[to, HEAD_SIZE:, :] = jnp.concatenate(stats + [empty], axis=0)


def output_kernel(partials, own_weight, pair_weight, out):
    at_row = lax.broadcasted_iota(jnp.int32, (HEAD_SIZE, HEAD_SIZE), 0)
    at_lane = lax.broadcasted_iota(jnp.int32, (HEAD_SIZE, HEAD_SIZE), 1)
    eye = (at_row == at_lane).astype(jnp.float32)
    peaks, totals = [], []
    for j in range(GROUP):
        stats = partials[j, HEAD_SIZE:, :].astype(jnp.float32)
        peaks.append(stats[0:1] + stats[1:2] + stats[2:3])
        totals.append(stats[3:4] + stats[4:5] + stats[5:6])
    peak = peaks[0]
    for p in peaks[1:]:
        peak = jnp.maximum(peak, p)
    fades = [jnp.exp2((p - peak) * EXP2_SCALE) for p in peaks]
    total = fades[0] * totals[0]
    for f, t in zip(fades[1:], totals[1:]):
        total += f * t
    attended = 0.0
    for j in range(GROUP):
        column = jnp.sum(eye * (fades[j] / total), axis=1, keepdims=True)
        attended += column * partials[j, :HEAD_SIZE, :].astype(jnp.float32)
    attended = attended.astype(jnp.bfloat16)
    even, odd = attended[: HEAD_SIZE // 2], attended[HEAD_SIZE // 2 :]
    is_odd = lax.rem(lax.axis_index("tp"), 2) == 1
    update = jnp.dot(
        jnp.where(is_odd, odd, even), own_weight[...], preferred_element_type=jnp.float32
    ) + jnp.dot(
        jnp.where(is_odd, even, odd), pair_weight[...], preferred_element_type=jnp.float32
    )
    out[...] = update.astype(jnp.bfloat16).reshape(out.shape)


def final_kernel(target, parts, out):
    update = parts[0].astype(jnp.float32)
    for i in range(1, parts.shape[0]):
        update += parts[i].astype(jnp.float32)
    out[...] = (target[...].astype(jnp.float32) + update).astype(jnp.bfloat16)


def call(kernel, outs, estimate, specs, scratch=(), vmem=48 * 1024 * 1024):
    return pl.pallas_call(
        kernel,
        out_shape=outs,
        in_specs=specs,
        scratch_shapes=list(scratch),
        out_specs=jax.tree.map(lambda _: VMEM, outs),
        cost_estimate=estimate,
        compiler_params=pltpu.CompilerParams(vmem_limit_bytes=vmem),
    )


def bf16(*shape):
    return jax.ShapeDtypeStruct(shape, jnp.bfloat16)


def body(
    target,
    source,
    target_gain,
    source_gain,
    query_weight,
    key_matrix,
    value_matrix,
    query_gain,
    key_gain,
    out_weight,
):
    width = target.shape[1]
    tp = lax.axis_size("tp")
    sp = lax.axis_size("sp")
    own_rows = target.shape[0]
    block = own_rows * tp
    source_rows = source.shape[0]
    halves = [[i + h * GROUP for i in range(GROUP)] for h in range(KEY_VALUE_HEADS)]
    parities = [[e + 2 * i for i in range(tp // 2)] for e in range(2)]
    along_z = [[2 * z + (z + core) % 2 for z in range(sp // 2)] for core in range(2)]
    side = math.isqrt(tp)
    opposite = [(i, (side - 1 - i // side) * side + i % side) for i in range(tp)]
    depth = width // 4

    own, other = call(
        key_value_kernel,
        (bf16(source_rows, 2 * HEAD_SIZE), bf16(source_rows, 2 * HEAD_SIZE)),
        cost(2 * source_rows * width * 512, 2400000),
        [VMEM, VMEM, HBM, HBM, VMEM],
        (
            pltpu.VMEM((4, depth, 2 * HEAD_SIZE), jnp.bfloat16),
            pltpu.VMEM((4, depth, 2 * HEAD_SIZE), jnp.bfloat16),
            pltpu.SemaphoreType.DMA((4, 2)),
        ),
        vmem=67043328,
    )(source, source_gain.reshape(1, width), key_matrix, value_matrix, key_gain)
    received = lax.ppermute(other, "tp", opposite)
    everyone = lax.all_to_all(
        jnp.broadcast_to(target, (tp, own_rows, width)), "tp", 0, 0, tiled=True
    ).reshape(block, width)
    near = lax.all_gather(
        jnp.concatenate([own, received], axis=0),
        "sp",
        axis=0,
        tiled=True,
        axis_index_groups=along_z,
    )
    copies = call(
        query_kernel,
        bf16(GROUP, block, HEAD_SIZE),
        cost(2 * block * width * HEAD_SIZE, 1400000),
        [VMEM] * 4,
    )(everyone, target_gain.reshape(1, width), query_weight, query_gain)
    all_queries = lax.all_to_all(
        copies, "tp", 0, 0, tiled=True, axis_index_groups=halves
    )
    far = lax.ppermute(near, "sp", [(i, i ^ 1) for i in range(sp)])
    pair_weight = lax.ppermute(out_weight, "tp", [(i, i ^ 1) for i in range(tp)])
    keys = 2 * near.shape[0]
    partials = call(
        attention_kernel,
        bf16(GROUP, block + STAT_ROWS, HEAD_SIZE),
        cost(4 * GROUP * block * keys * HEAD_SIZE, 2500000, GROUP * block * keys),
        [VMEM] * 3,
    )(all_queries, near, far)
    mine = lax.all_to_all(partials, "tp", 0, 0, tiled=True, axis_index_groups=halves)
    update = call(
        output_kernel,
        bf16(tp // 2, own_rows, width),
        cost(2 * block * width * HEAD_SIZE, 1900000),
        [VMEM] * 3,
    )(mine, out_weight, pair_weight)
    parts = lax.all_to_all(update, "tp", 0, 0, tiled=True, axis_index_groups=parities)
    return call(
        final_kernel,
        bf16(own_rows, width),
        cost(tp // 2 * own_rows * width, 300000),
        [VMEM] * 2,
    )(target, parts)


def solution(mesh):
    return jax.shard_map(
        body,
        mesh=mesh,
        in_specs=(
            P(("sp", "tp"), None),
            P(("sp", "tp"), None),
            P(),
            P(),
            P(None, "tp"),
            P(),
            P(),
            P("tp", None),
            P(),
            P("tp", None),
        ),
        out_specs=P(("sp", "tp"), None),
        check_vma=False,
    )
```

```python
import math

import jax
import jax.numpy as jnp
from jax import lax
from jax.experimental import pallas as pl
from jax.experimental.pallas import tpu as pltpu
from jax.sharding import PartitionSpec as P


QUERY_HEAD_COUNT = 16
KEY_VALUE_HEADS = 2
HEAD_SIZE = 128
GROUP = QUERY_HEAD_COUNT // KEY_VALUE_HEADS
EPSILON = 1e-06
EXP2_SCALE = math.log2(math.e) / math.sqrt(HEAD_SIZE)
STAT_ROWS = 16

VMEM = pl.BlockSpec(memory_space=pltpu.VMEM)
HBM = pl.BlockSpec(memory_space=pltpu.HBM)


def cost(flops, nbytes, transcendentals=0):
    return pl.CostEstimate(
        flops=flops, bytes_accessed=nbytes, transcendentals=transcendentals
    )


def normed(values_in, gain):
    return (
        values_in
        * lax.rsqrt(jnp.mean(values_in * values_in, axis=-1, keepdims=True) + EPSILON)
        * gain
    )


def key_value_kernel(
    target,
    source,
    gain,
    key_matrix,
    value_matrix,
    key_gain,
    own,
    other,
    target_copies,
    target_here,
    source_here,
    gain_here,
    key_gain_here,
    key_part,
    value_part,
    arrived,
    matrix_arrived,
    left,
):
    depth = key_part.shape[1]
    parts = key_part.shape[0]
    inputs = [
        pltpu.make_async_copy(a, b, arrived.at[i])
        for i, (a, b) in enumerate(
            (
                (target, target_here),
                (source, source_here),
                (gain, gain_here),
                (key_gain, key_gain_here),
            )
        )
    ]
    matrices = [
        pltpu.make_async_copy(
            matrix.at[pl.ds(i * depth, depth), :], buffer.at[i], matrix_arrived.at[i, j]
        )
        for i in range(parts)
        for j, (matrix, buffer) in enumerate(
            ((key_matrix, key_part), (value_matrix, value_part))
        )
    ]
    outputs = [
        pltpu.make_async_copy(target_here, target_copies.at[i], left.at[i])
        for i in range(target_copies.shape[0])
    ]
    for c in inputs + matrices:
        c.start()
    inputs[0].wait()
    for c in outputs:
        c.start()
    second = lax.axis_index("tp") >= GROUP
    for c in inputs[1:]:
        c.wait()
    rows = normed(source_here[...].astype(jnp.float32), gain_here[...])
    rows = rows.astype(jnp.bfloat16)
    raw, values = 0.0, 0.0
    for i in range(parts):
        matrices[2 * i].wait()
        matrices[2 * i + 1].wait()
        part = rows[:, i * depth : (i + 1) * depth]
        raw += jnp.dot(part, key_part[i], preferred_element_type=jnp.float32)
        values += jnp.dot(part, value_part[i], preferred_element_type=jnp.float32)
    values = values.astype(jnp.bfloat16)
    heads = []
    for h in range(KEY_VALUE_HEADS):
        at = slice(h * HEAD_SIZE, (h + 1) * HEAD_SIZE)
        keys = normed(raw[:, at], key_gain_here[h : h + 1, :]).astype(jnp.bfloat16)
        heads.append(jnp.concatenate([keys, values[:, at]], axis=1))
    own[...] = jnp.where(second, heads[1], heads[0])
    other[...] = jnp.where(second, heads[0], heads[1])
    for c in outputs:
        c.wait()


def query_kernel(target, gain, weight, head_gain, copies):
    rows = normed(target[...].astype(jnp.float32), gain[...]).astype(jnp.bfloat16)
    raw = jnp.dot(rows, weight[...], preferred_element_type=jnp.float32)
    queries = normed(raw, head_gain[...]).astype(jnp.bfloat16)
    for i in range(GROUP):
        copies[i] = queries


def in_three(x):
    first = x.astype(jnp.bfloat16)
    rest = x - first.astype(jnp.float32)
    second = rest.astype(jnp.bfloat16)
    third = (rest - second.astype(jnp.float32)).astype(jnp.bfloat16)
    return [first, second, third]


TILE = 2 * HEAD_SIZE


def scores_of(queries, kv, tile):
    q = queries[tile * 2 : tile * 2 + 2].reshape(TILE, HEAD_SIZE)
    return lax.dot_general(
        q,
        kv[:, :HEAD_SIZE],
        (((1,), (1,)), ((), ())),
        preferred_element_type=jnp.float32,
    )


def weighed(scores, peak, kv):
    weights = jnp.exp2((scores - peak) * EXP2_SCALE)
    return (
        jnp.sum(weights, axis=-1, keepdims=True),
        jnp.dot(
            weights.astype(jnp.bfloat16),
            kv[:, HEAD_SIZE:],
            preferred_element_type=jnp.float32,
        ),
    )


def near_kernel(queries, kv, peaks, totals, sums):
    for tile in range(GROUP // 2):
        scores = scores_of(queries, kv, tile)
        peak = jnp.max(scores, axis=-1, keepdims=True)
        total, weighted = weighed(scores, peak, kv)
        peaks[tile] = jnp.broadcast_to(peak, (TILE, HEAD_SIZE))
        totals[tile] = jnp.broadcast_to(total, (TILE, HEAD_SIZE))
        sums[tile] = weighted


def far_kernel(queries, kv, peaks, totals, sums, out):
    at_row = lax.broadcasted_iota(jnp.int32, (HEAD_SIZE, HEAD_SIZE), 0)
    at_lane = lax.broadcasted_iota(jnp.int32, (HEAD_SIZE, HEAD_SIZE), 1)
    eye = (at_row == at_lane).astype(jnp.float32)

    def as_row(columns):
        return jnp.sum(eye * columns, axis=0, keepdims=True)

    for tile in range(GROUP // 2):
        scores = scores_of(queries, kv, tile)
        peak = jnp.maximum(peaks[tile], jnp.max(scores, axis=-1, keepdims=True))
        fade = jnp.exp2((peaks[tile] - peak) * EXP2_SCALE)
        total, weighted = weighed(scores, peak[:, :1], kv)
        total = totals[tile] * fade + total
        weighted = sums[tile] * fade + weighted
        for odd in range(2):
            def picked(columns):
                return jnp.concatenate(
                    [columns[i : i + 8] for i in range(8 * odd, TILE, 16)], axis=0
                )

            to = tile * 2 + odd
            out[to, :HEAD_SIZE, :] = picked(weighted).astype(jnp.bfloat16)
            stats = in_three(as_row(picked(peak))) + in_three(as_row(picked(total)))
            empty = jnp.zeros((STAT_ROWS - len(stats), HEAD_SIZE), jnp.bfloat16)
            out[to, HEAD_SIZE:, :] = jnp.concatenate(stats + [empty], axis=0)


def output_kernel(partials, own_weight, pair_weight, out):
    at_row = lax.broadcasted_iota(jnp.int32, (HEAD_SIZE, HEAD_SIZE), 0)
    at_lane = lax.broadcasted_iota(jnp.int32, (HEAD_SIZE, HEAD_SIZE), 1)
    eye = (at_row == at_lane).astype(jnp.float32)
    peaks, totals = [], []
    for j in range(GROUP):
        stats = partials[j, HEAD_SIZE:, :].astype(jnp.float32)
        peaks.append(stats[0:1] + stats[1:2] + stats[2:3])
        totals.append(stats[3:4] + stats[4:5] + stats[5:6])
    peak = peaks[0]
    for p in peaks[1:]:
        peak = jnp.maximum(peak, p)
    fades = [jnp.exp2((p - peak) * EXP2_SCALE) for p in peaks]
    total = fades[0] * totals[0]
    for f, t in zip(fades[1:], totals[1:]):
        total += f * t
    attended = 0.0
    for j in range(GROUP):
        column = jnp.sum(eye * (fades[j] / total), axis=1, keepdims=True)
        attended += column * partials[j, :HEAD_SIZE, :].astype(jnp.float32)
    attended = attended.astype(jnp.bfloat16)
    even, odd = attended[: HEAD_SIZE // 2], attended[HEAD_SIZE // 2 :]
    is_odd = lax.rem(lax.axis_index("tp"), 2) == 1
    update = jnp.dot(
        jnp.where(is_odd, odd, even), own_weight[...], preferred_element_type=jnp.float32
    ) + jnp.dot(
        jnp.where(is_odd, even, odd), pair_weight[...], preferred_element_type=jnp.float32
    )
    out[...] = update.astype(jnp.bfloat16).reshape(out.shape)


def final_kernel(target, parts, out):
    update = parts[0].astype(jnp.float32)
    for i in range(1, parts.shape[0]):
        update += parts[i].astype(jnp.float32)
    out[...] = (target[...].astype(jnp.float32) + update).astype(jnp.bfloat16)


def call(kernel, outs, estimate, specs, out_specs=None, scratch=(), vmem=48 * 1024 * 1024):
    return pl.pallas_call(
        kernel,
        out_shape=outs,
        in_specs=specs,
        scratch_shapes=list(scratch),
        out_specs=out_specs or jax.tree.map(lambda _: VMEM, outs),
        cost_estimate=estimate,
        compiler_params=pltpu.CompilerParams(vmem_limit_bytes=vmem),
    )


def bf16(*shape):
    return jax.ShapeDtypeStruct(shape, jnp.bfloat16)


def body(
    target,
    source,
    target_gain,
    source_gain,
    query_weight,
    key_matrix,
    value_matrix,
    query_gain,
    key_gain,
    out_weight,
):
    width = target.shape[1]
    tp = lax.axis_size("tp")
    sp = lax.axis_size("sp")
    own_rows = target.shape[0]
    block = own_rows * tp
    source_rows = source.shape[0]
    halves = [[i + h * GROUP for i in range(GROUP)] for h in range(KEY_VALUE_HEADS)]
    parities = [[e + 2 * i for i in range(tp // 2)] for e in range(2)]
    along_z = [[2 * z + (z + core) % 2 for z in range(sp // 2)] for core in range(2)]
    side = math.isqrt(tp)
    opposite = [(i, (side - 1 - i // side) * side + i % side) for i in range(tp)]
    depth = width // 4

    own, other, target_copies = call(
        key_value_kernel,
        (
            bf16(source_rows, 2 * HEAD_SIZE),
            bf16(source_rows, 2 * HEAD_SIZE),
            bf16(tp, own_rows, width),
        ),
        cost(2 * source_rows * width * 512, 3000000),
        [HBM] * 6,
        (VMEM, VMEM, HBM),
        (
            pltpu.VMEM((own_rows, width), jnp.bfloat16),
            pltpu.VMEM((source_rows, width), jnp.bfloat16),
            pltpu.VMEM((1, width), jnp.float32),
            pltpu.VMEM((KEY_VALUE_HEADS, HEAD_SIZE), jnp.float32),
            pltpu.VMEM((4, depth, 2 * HEAD_SIZE), jnp.bfloat16),
            pltpu.VMEM((4, depth, 2 * HEAD_SIZE), jnp.bfloat16),
            pltpu.SemaphoreType.DMA((4,)),
            pltpu.SemaphoreType.DMA((4, 2)),
            pltpu.SemaphoreType.DMA((tp,)),
        ),
        vmem=67043328,
    )(target, source, source_gain.reshape(1, width), key_matrix, value_matrix, key_gain)
    everyone = lax.all_to_all(target_copies, "tp", 0, 0, tiled=True)
    everyone = everyone.reshape(block, width)
    received = lax.ppermute(other, "tp", opposite)
    pair_weight = lax.ppermute(out_weight, "tp", [(i, i ^ 1) for i in range(tp)])
    copies = call(
        query_kernel,
        bf16(GROUP, block, HEAD_SIZE),
        cost(2 * block * width * HEAD_SIZE, 1400000),
        [VMEM] * 4,
    )(everyone, target_gain.reshape(1, width), query_weight, query_gain)
    all_queries = lax.all_to_all(
        copies, "tp", 0, 0, tiled=True, axis_index_groups=halves
    )
    near = lax.all_gather(
        jnp.concatenate([own, received], axis=0),
        "sp",
        axis=0,
        tiled=True,
        axis_index_groups=along_z,
    )
    far = lax.ppermute(near, "sp", [(i, i ^ 1) for i in range(sp)])
    keys = near.shape[0]
    work = cost(
        4 * GROUP * block * keys * HEAD_SIZE, 2500000, GROUP * block * keys
    )
    carried = jax.ShapeDtypeStruct((GROUP // 2, TILE, HEAD_SIZE), jnp.float32)
    state = call(near_kernel, (carried,) * 3, work, [VMEM] * 2)(all_queries, near)
    partials = call(
        far_kernel, bf16(GROUP, block + STAT_ROWS, HEAD_SIZE), work, [VMEM] * 5
    )(all_queries, far, *state)
    mine = lax.all_to_all(partials, "tp", 0, 0, tiled=True, axis_index_groups=halves)
    update = call(
        output_kernel,
        bf16(tp // 2, own_rows, width),
        cost(2 * block * width * HEAD_SIZE, 1900000),
        [VMEM] * 3,
    )(mine, out_weight, pair_weight)
    parts = lax.all_to_all(update, "tp", 0, 0, tiled=True, axis_index_groups=parities)
    return call(
        final_kernel,
        bf16(own_rows, width),
        cost(tp // 2 * own_rows * width, 300000),
        [VMEM] * 2,
    )(target, parts)


def solution(mesh):
    return jax.shard_map(
        body,
        mesh=mesh,
        in_specs=(
            P(("sp", "tp"), None),
            P(("sp", "tp"), None),
            P(),
            P(),
            P(None, "tp"),
            P(),
            P(),
            P("tp", None),
            P(),
            P("tp", None),
        ),
        out_specs=P(("sp", "tp"), None),
        check_vma=False,
    )
```

```python
import math

import jax
import jax.numpy as jnp
from jax import lax
from jax.experimental import pallas as pl
from jax.experimental.pallas import tpu as pltpu
from jax.sharding import PartitionSpec as P


QUERY_HEAD_COUNT = 16
KEY_VALUE_HEADS = 2
HEAD_SIZE = 128
GROUP = QUERY_HEAD_COUNT // KEY_VALUE_HEADS
EPSILON = 1e-06
EXP2_SCALE = math.log2(math.e) / math.sqrt(HEAD_SIZE)
STAT_ROWS = 16

VMEM = pl.BlockSpec(memory_space=pltpu.VMEM)
HBM = pl.BlockSpec(memory_space=pltpu.HBM)


def cost(flops, nbytes, transcendentals=0):
    return pl.CostEstimate(
        flops=flops, bytes_accessed=nbytes, transcendentals=transcendentals
    )


def normed(values_in, gain):
    return (
        values_in
        * lax.rsqrt(jnp.mean(values_in * values_in, axis=-1, keepdims=True) + EPSILON)
        * gain
    )


def key_value_kernel(
    target,
    source,
    gain,
    key_matrix,
    value_matrix,
    key_gain,
    target_gain,
    query_gain,
    own,
    other,
    target_copies,
    target_gain_here,
    query_gain_here,
    target_here,
    source_here,
    gain_here,
    key_gain_here,
    key_part,
    value_part,
    arrived,
    matrix_arrived,
    left,
):
    depth = key_part.shape[1]
    parts = key_part.shape[0]
    inputs = [
        pltpu.make_async_copy(a, b, arrived.at[i])
        for i, (a, b) in enumerate(
            (
                (target, target_here),
                (source, source_here),
                (gain, gain_here),
                (key_gain, key_gain_here),
                (target_gain, target_gain_here),
                (query_gain, query_gain_here),
            )
        )
    ]
    matrices = [
        pltpu.make_async_copy(
            matrix.at[pl.ds(i * depth, depth), :], buffer.at[i], matrix_arrived.at[i, j]
        )
        for i in range(parts)
        for j, (matrix, buffer) in enumerate(
            ((key_matrix, key_part), (value_matrix, value_part))
        )
    ]
    outputs = [
        pltpu.make_async_copy(target_here, target_copies.at[i], left.at[i])
        for i in range(target_copies.shape[0])
    ]
    for c in inputs + matrices:
        c.start()
    inputs[0].wait()
    for c in outputs:
        c.start()
    second = lax.axis_index("tp") >= GROUP
    for c in inputs[1:]:
        c.wait()
    rows = normed(source_here[...].astype(jnp.float32), gain_here[...])
    rows = rows.astype(jnp.bfloat16)
    raw, values = 0.0, 0.0
    for i in range(parts):
        matrices[2 * i].wait()
        matrices[2 * i + 1].wait()
        part = rows[:, i * depth : (i + 1) * depth]
        raw += jnp.dot(part, key_part[i], preferred_element_type=jnp.float32)
        values += jnp.dot(part, value_part[i], preferred_element_type=jnp.float32)
    values = values.astype(jnp.bfloat16)
    heads = []
    for h in range(KEY_VALUE_HEADS):
        at = slice(h * HEAD_SIZE, (h + 1) * HEAD_SIZE)
        keys = normed(raw[:, at], key_gain_here[h : h + 1, :]).astype(jnp.bfloat16)
        heads.append(jnp.concatenate([keys, values[:, at]], axis=1))
    own[...] = jnp.where(second, heads[1], heads[0])
    other[...] = jnp.where(second, heads[0], heads[1])
    for c in outputs:
        c.wait()


def query_kernel(target, gain, weight, head_gain, copies):
    rows = normed(target[...].astype(jnp.float32), gain[...]).astype(jnp.bfloat16)
    raw = jnp.dot(rows, weight[...], preferred_element_type=jnp.float32)
    queries = normed(raw, head_gain[...]).astype(jnp.bfloat16)
    for i in range(GROUP):
        copies[i] = queries


def in_three(x):
    first = x.astype(jnp.bfloat16)
    rest = x - first.astype(jnp.float32)
    second = rest.astype(jnp.bfloat16)
    third = (rest - second.astype(jnp.float32)).astype(jnp.bfloat16)
    return [first, second, third]


def attention_kernel(queries, near, far, out):
    per_tile = 2
    rows = per_tile * HEAD_SIZE
    at_row = lax.broadcasted_iota(jnp.int32, (HEAD_SIZE, HEAD_SIZE), 0)
    at_lane = lax.broadcasted_iota(jnp.int32, (HEAD_SIZE, HEAD_SIZE), 1)
    eye = (at_row == at_lane).astype(jnp.float32)

    def as_row(column):
        return jnp.sum(eye * column, axis=0, keepdims=True)

    for tile in range(GROUP // per_tile):
        q = queries[tile * per_tile : (tile + 1) * per_tile].reshape(rows, HEAD_SIZE)
        scores = [
            lax.dot_general(
                q,
                kv[:, :HEAD_SIZE],
                (((1,), (1,)), ((), ())),
                preferred_element_type=jnp.float32,
            )
            for kv in (near, far)
        ]
        peak = jnp.maximum(
            jnp.max(scores[0], axis=-1, keepdims=True),
            jnp.max(scores[1], axis=-1, keepdims=True),
        )
        total, weighted = 0.0, 0.0
        for kv, s in zip((near, far), scores):
            weights = jnp.exp2((s - peak) * EXP2_SCALE)
            total += jnp.sum(weights, axis=-1, keepdims=True)
            weighted += jnp.dot(
                weights.astype(jnp.bfloat16),
                kv[:, HEAD_SIZE:],
                preferred_element_type=jnp.float32,
            )
        for odd in range(2):
            def picked(column):
                return jnp.concatenate(
                    [column[i : i + 8] for i in range(8 * odd, rows, 16)], axis=0
                )

            to = tile * 2 + odd
            out[to, :HEAD_SIZE, :] = picked(weighted).astype(jnp.bfloat16)
            stats = in_three(as_row(picked(peak))) + in_three(as_row(picked(total)))
            empty = jnp.zeros((STAT_ROWS - len(stats), HEAD_SIZE), jnp.bfloat16)
            out[to, HEAD_SIZE:, :] = jnp.concatenate(stats + [empty], axis=0)


def output_kernel(partials, own_weight, pair_weight, out):
    at_row = lax.broadcasted_iota(jnp.int32, (HEAD_SIZE, HEAD_SIZE), 0)
    at_lane = lax.broadcasted_iota(jnp.int32, (HEAD_SIZE, HEAD_SIZE), 1)
    eye = (at_row == at_lane).astype(jnp.float32)
    peaks, totals = [], []
    for j in range(GROUP):
        stats = partials[j, HEAD_SIZE:, :].astype(jnp.float32)
        peaks.append(stats[0:1] + stats[1:2] + stats[2:3])
        totals.append(stats[3:4] + stats[4:5] + stats[5:6])
    peak = peaks[0]
    for p in peaks[1:]:
        peak = jnp.maximum(peak, p)
    fades = [jnp.exp2((p - peak) * EXP2_SCALE) for p in peaks]
    total = fades[0] * totals[0]
    for f, t in zip(fades[1:], totals[1:]):
        total += f * t
    attended = 0.0
    for j in range(GROUP):
        column = jnp.sum(eye * (fades[j] / total), axis=1, keepdims=True)
        attended += column * partials[j, :HEAD_SIZE, :].astype(jnp.float32)
    attended = attended.astype(jnp.bfloat16)
    even, odd = attended[: HEAD_SIZE // 2], attended[HEAD_SIZE // 2 :]
    is_odd = lax.rem(lax.axis_index("tp"), 2) == 1
    update = jnp.dot(
        jnp.where(is_odd, odd, even), own_weight[...], preferred_element_type=jnp.float32
    ) + jnp.dot(
        jnp.where(is_odd, even, odd), pair_weight[...], preferred_element_type=jnp.float32
    )
    out[...] = update.astype(jnp.bfloat16).reshape(out.shape)


def final_kernel(target, parts, out):
    update = parts[0].astype(jnp.float32)
    for i in range(1, parts.shape[0]):
        update += parts[i].astype(jnp.float32)
    out[...] = (target[...].astype(jnp.float32) + update).astype(jnp.bfloat16)


def call(kernel, outs, estimate, specs, out_specs=None, scratch=(), vmem=48 * 1024 * 1024):
    return pl.pallas_call(
        kernel,
        out_shape=outs,
        in_specs=specs,
        scratch_shapes=list(scratch),
        out_specs=out_specs or jax.tree.map(lambda _: VMEM, outs),
        cost_estimate=estimate,
        compiler_params=pltpu.CompilerParams(vmem_limit_bytes=vmem),
    )


def bf16(*shape):
    return jax.ShapeDtypeStruct(shape, jnp.bfloat16)


def body(
    target,
    source,
    target_gain,
    source_gain,
    query_weight,
    key_matrix,
    value_matrix,
    query_gain,
    key_gain,
    out_weight,
):
    width = target.shape[1]
    tp = lax.axis_size("tp")
    sp = lax.axis_size("sp")
    own_rows = target.shape[0]
    block = own_rows * tp
    source_rows = source.shape[0]
    halves = [[i + h * GROUP for i in range(GROUP)] for h in range(KEY_VALUE_HEADS)]
    parities = [[e + 2 * i for i in range(tp // 2)] for e in range(2)]
    along_z = [[2 * z + (z + core) % 2 for z in range(sp // 2)] for core in range(2)]
    side = math.isqrt(tp)
    opposite = [(i, (side - 1 - i // side) * side + i % side) for i in range(tp)]
    depth = width // 4

    pieces = (source_rows, 2 * HEAD_SIZE)
    own, other, target_copies, target_gain_here, query_gain_here = call(
        key_value_kernel,
        (
            pltpu.VMEM(pieces, jnp.bfloat16),
            pltpu.VMEM(pieces, jnp.bfloat16),
            pltpu.HBM((tp, own_rows, width), jnp.bfloat16),
            pltpu.VMEM((1, width), jnp.float32),
            pltpu.VMEM((1, HEAD_SIZE), jnp.float32),
        ),
        cost(2 * source_rows * width * 512, 3000000),
        [HBM] * 8,
        (VMEM, VMEM, HBM, VMEM, VMEM),
        (
            pltpu.VMEM((own_rows, width), jnp.bfloat16),
            pltpu.VMEM((source_rows, width), jnp.bfloat16),
            pltpu.VMEM((1, width), jnp.float32),
            pltpu.VMEM((KEY_VALUE_HEADS, HEAD_SIZE), jnp.float32),
            pltpu.VMEM((4, depth, 2 * HEAD_SIZE), jnp.bfloat16),
            pltpu.VMEM((4, depth, 2 * HEAD_SIZE), jnp.bfloat16),
            pltpu.SemaphoreType.DMA((6,)),
            pltpu.SemaphoreType.DMA((4, 2)),
            pltpu.SemaphoreType.DMA((tp,)),
        ),
        vmem=16 * 1024 * 1024,
    )(
        *(
            pltpu.with_memory_space_constraint(x, pltpu.HBM)
            for x in (
                target,
                source,
                source_gain.reshape(1, width),
                key_matrix,
                value_matrix,
                key_gain,
                target_gain.reshape(1, width),
                query_gain,
            )
        )
    )
    received = lax.ppermute(other, "tp", opposite)
    everyone = lax.all_to_all(target_copies, "tp", 0, 0, tiled=True)
    everyone = everyone.reshape(block, width)
    near = lax.all_gather(
        jnp.concatenate([own, received], axis=0),
        "sp",
        axis=0,
        tiled=True,
        axis_index_groups=along_z,
    )
    copies = call(
        query_kernel,
        bf16(GROUP, block, HEAD_SIZE),
        cost(2 * block * width * HEAD_SIZE, 1400000),
        [VMEM] * 4,
    )(everyone, target_gain_here, query_weight, query_gain_here)
    all_queries = lax.all_to_all(
        copies, "tp", 0, 0, tiled=True, axis_index_groups=halves
    )
    far = lax.ppermute(near, "sp", [(i, i ^ 1) for i in range(sp)])
    pair_weight = lax.ppermute(out_weight, "tp", [(i, i ^ 1) for i in range(tp)])
    keys = 2 * near.shape[0]
    partials = call(
        attention_kernel,
        bf16(GROUP, block + STAT_ROWS, HEAD_SIZE),
        cost(4 * GROUP * block * keys * HEAD_SIZE, 2500000, GROUP * block * keys),
        [VMEM] * 3,
    )(all_queries, near, far)
    mine = lax.all_to_all(partials, "tp", 0, 0, tiled=True, axis_index_groups=halves)
    update = call(
        output_kernel,
        bf16(tp // 2, own_rows, width),
        cost(2 * block * width * HEAD_SIZE, 1900000),
        [VMEM] * 3,
    )(mine, out_weight, pair_weight)
    parts = lax.all_to_all(update, "tp", 0, 0, tiled=True, axis_index_groups=parities)
    return call(
        final_kernel,
        bf16(own_rows, width),
        cost(tp // 2 * own_rows * width, 300000),
        [VMEM] * 2,
    )(target, parts)


def solution(mesh):
    return jax.shard_map(
        body,
        mesh=mesh,
        in_specs=(
            P(("sp", "tp"), None),
            P(("sp", "tp"), None),
            P(),
            P(),
            P(None, "tp"),
            P(),
            P(),
            P("tp", None),
            P(),
            P("tp", None),
        ),
        out_specs=P(("sp", "tp"), None),
        check_vma=False,
    )
```

```python
import math

import jax
import jax.numpy as jnp
from jax import lax
from jax.experimental import pallas as pl
from jax.experimental.pallas import tpu as pltpu
from jax.sharding import PartitionSpec as P


QUERY_HEAD_COUNT = 16
KEY_VALUE_HEADS = 2
HEAD_SIZE = 128
GROUP = QUERY_HEAD_COUNT // KEY_VALUE_HEADS
EPSILON = 1e-06
EXP2_SCALE = math.log2(math.e) / math.sqrt(HEAD_SIZE)
STAT_ROWS = 16

VMEM = pl.BlockSpec(memory_space=pltpu.VMEM)
HBM = pl.BlockSpec(memory_space=pltpu.HBM)


def cost(flops, nbytes, transcendentals=0):
    return pl.CostEstimate(
        flops=flops, bytes_accessed=nbytes, transcendentals=transcendentals
    )


def normed(values_in, gain):
    return (
        values_in
        * lax.rsqrt(jnp.mean(values_in * values_in, axis=-1, keepdims=True) + EPSILON)
        * gain
    )


def key_value_kernel(
    target,
    source,
    gain,
    key_matrix,
    value_matrix,
    key_gain,
    target_gain,
    query_gain,
    own,
    other,
    target_copies,
    target_gain_here,
    query_gain_here,
    target_here,
    source_here,
    gain_here,
    key_gain_here,
    key_part,
    value_part,
    arrived,
    matrix_arrived,
    left,
):
    depth = key_part.shape[1]
    parts = key_part.shape[0]
    inputs = [
        pltpu.make_async_copy(a, b, arrived.at[i])
        for i, (a, b) in enumerate(
            (
                (target, target_here),
                (source, source_here),
                (gain, gain_here),
                (key_gain, key_gain_here),
                (target_gain, target_gain_here),
                (query_gain, query_gain_here),
            )
        )
    ]
    matrices = [
        pltpu.make_async_copy(
            matrix.at[pl.ds(i * depth, depth), :], buffer.at[i], matrix_arrived.at[i, j]
        )
        for i in range(parts)
        for j, (matrix, buffer) in enumerate(
            ((key_matrix, key_part), (value_matrix, value_part))
        )
    ]
    outputs = [
        pltpu.make_async_copy(target_here, target_copies.at[i], left.at[i])
        for i in range(target_copies.shape[0])
    ]
    for c in inputs + matrices:
        c.start()
    inputs[0].wait()
    for c in outputs:
        c.start()
    second = lax.axis_index("tp") >= GROUP
    for c in inputs[1:]:
        c.wait()
    rows = normed(source_here[...].astype(jnp.float32), gain_here[...])
    rows = rows.astype(jnp.bfloat16)
    raw, values = 0.0, 0.0
    for i in range(parts):
        matrices[2 * i].wait()
        matrices[2 * i + 1].wait()
        part = rows[:, i * depth : (i + 1) * depth]
        raw += jnp.dot(part, key_part[i], preferred_element_type=jnp.float32)
        values += jnp.dot(part, value_part[i], preferred_element_type=jnp.float32)
    values = values.astype(jnp.bfloat16)
    heads = []
    for h in range(KEY_VALUE_HEADS):
        at = slice(h * HEAD_SIZE, (h + 1) * HEAD_SIZE)
        keys = normed(raw[:, at], key_gain_here[h : h + 1, :]).astype(jnp.bfloat16)
        heads.append(jnp.concatenate([keys, values[:, at]], axis=1))
    own[...] = jnp.where(second, heads[1], heads[0])
    other[...] = jnp.where(second, heads[0], heads[1])
    for c in outputs:
        c.wait()


def query_kernel(target, gain, weight, head_gain, copies, here, left):
    rows = normed(target[...].astype(jnp.float32), gain[...]).astype(jnp.bfloat16)
    raw = jnp.dot(rows, weight[...], preferred_element_type=jnp.float32)
    here[...] = normed(raw, head_gain[...]).astype(jnp.bfloat16)
    outputs = [
        pltpu.make_async_copy(here, copies.at[i], left.at[i]) for i in range(GROUP)
    ]
    for c in outputs:
        c.start()
    for c in outputs:
        c.wait()


def in_three(x):
    first = x.astype(jnp.bfloat16)
    rest = x - first.astype(jnp.float32)
    second = rest.astype(jnp.bfloat16)
    third = (rest - second.astype(jnp.float32)).astype(jnp.bfloat16)
    return [first, second, third]


def attention_kernel(queries, near, far, out, here, left):
    rows = 2 * HEAD_SIZE
    at_row = lax.broadcasted_iota(jnp.int32, (HEAD_SIZE, HEAD_SIZE), 0)
    at_lane = lax.broadcasted_iota(jnp.int32, (HEAD_SIZE, HEAD_SIZE), 1)
    eye = (at_row == at_lane).astype(jnp.float32)

    def as_row(column):
        return jnp.sum(eye * column, axis=0, keepdims=True)

    outputs = []
    for head in range(GROUP):
        if head % 4 >= 2:
            continue
        q = jnp.concatenate([queries[head], queries[head + 2]], axis=0)
        scores = [
            lax.dot_general(
                q,
                kv[:, :HEAD_SIZE],
                (((1,), (1,)), ((), ())),
                preferred_element_type=jnp.float32,
            )
            for kv in (near, far)
        ]
        peak = jnp.maximum(
            jnp.max(scores[0], axis=-1, keepdims=True),
            jnp.max(scores[1], axis=-1, keepdims=True),
        )
        total, weighted = 0.0, 0.0
        for kv, s in zip((near, far), scores):
            weights = jnp.exp2((s - peak) * EXP2_SCALE)
            total += jnp.sum(weights, axis=-1, keepdims=True)
            weighted += jnp.dot(
                weights.astype(jnp.bfloat16),
                kv[:, HEAD_SIZE:],
                preferred_element_type=jnp.float32,
            )
        for side in range(2):
            def picked(column):
                return jnp.concatenate(
                    [column[i : i + 16] for i in range(16 * side, rows, 32)], axis=0
                )

            to = head + 2 * side
            here[to, :HEAD_SIZE, :] = picked(weighted).astype(jnp.bfloat16)
            stats = in_three(as_row(picked(peak))) + in_three(as_row(picked(total)))
            empty = jnp.zeros((STAT_ROWS - len(stats), HEAD_SIZE), jnp.bfloat16)
            here[to, HEAD_SIZE:, :] = jnp.concatenate(stats + [empty], axis=0)
            outputs.append(pltpu.make_async_copy(here.at[to], out.at[to], left.at[to]))
            outputs[-1].start()
    for c in outputs:
        c.wait()


def output_kernel(partials, own_weight, pair_weight, out):
    at_row = lax.broadcasted_iota(jnp.int32, (HEAD_SIZE, HEAD_SIZE), 0)
    at_lane = lax.broadcasted_iota(jnp.int32, (HEAD_SIZE, HEAD_SIZE), 1)
    eye = (at_row == at_lane).astype(jnp.float32)
    peaks, totals = [], []
    for j in range(GROUP):
        stats = partials[j, HEAD_SIZE:, :].astype(jnp.float32)
        peaks.append(stats[0:1] + stats[1:2] + stats[2:3])
        totals.append(stats[3:4] + stats[4:5] + stats[5:6])
    peak = peaks[0]
    for p in peaks[1:]:
        peak = jnp.maximum(peak, p)
    fades = [jnp.exp2((p - peak) * EXP2_SCALE) for p in peaks]
    total = fades[0] * totals[0]
    for f, t in zip(fades[1:], totals[1:]):
        total += f * t
    attended = 0.0
    for j in range(GROUP):
        column = jnp.sum(eye * (fades[j] / total), axis=1, keepdims=True)
        attended += column * partials[j, :HEAD_SIZE, :].astype(jnp.float32)
    attended = attended.astype(jnp.bfloat16)
    low, high = attended[: HEAD_SIZE // 2], attended[HEAD_SIZE // 2 :]
    is_high = lax.rem(lax.axis_index("tp"), 4) >= 2
    update = jnp.dot(
        jnp.where(is_high, high, low), own_weight[...], preferred_element_type=jnp.float32
    ) + jnp.dot(
        jnp.where(is_high, low, high), pair_weight[...], preferred_element_type=jnp.float32
    )
    out[...] = update.astype(jnp.bfloat16).reshape(out.shape)


def final_kernel(target, parts, out):
    update = parts[0].astype(jnp.float32)
    for i in range(1, parts.shape[0]):
        update += parts[i].astype(jnp.float32)
    out[...] = (target[...].astype(jnp.float32) + update).astype(jnp.bfloat16)


def call(kernel, outs, estimate, specs, out_specs=None, scratch=(), vmem=48 * 1024 * 1024):
    return pl.pallas_call(
        kernel,
        out_shape=outs,
        in_specs=specs,
        scratch_shapes=list(scratch),
        out_specs=out_specs or jax.tree.map(lambda _: VMEM, outs),
        cost_estimate=estimate,
        compiler_params=pltpu.CompilerParams(vmem_limit_bytes=vmem),
    )


def bf16(*shape):
    return jax.ShapeDtypeStruct(shape, jnp.bfloat16)


def body(
    target,
    source,
    target_gain,
    source_gain,
    query_weight,
    key_matrix,
    value_matrix,
    query_gain,
    key_gain,
    out_weight,
):
    width = target.shape[1]
    tp = lax.axis_size("tp")
    sp = lax.axis_size("sp")
    own_rows = target.shape[0]
    block = own_rows * tp
    source_rows = source.shape[0]
    halves = [[i + h * GROUP for i in range(GROUP)] for h in range(KEY_VALUE_HEADS)]
    sides = [[i for i in range(tp) if i // 2 % 2 == e] for e in range(2)]
    along_z = [[2 * z + (z + core) % 2 for z in range(sp // 2)] for core in range(2)]
    side = math.isqrt(tp)
    opposite = [(i, (side - 1 - i // side) * side + i % side) for i in range(tp)]
    depth = width // 4

    pieces = (source_rows, 2 * HEAD_SIZE)
    own, other, target_copies, target_gain_here, query_gain_here = call(
        key_value_kernel,
        (
            pltpu.VMEM(pieces, jnp.bfloat16),
            pltpu.VMEM(pieces, jnp.bfloat16),
            pltpu.HBM((tp, own_rows, width), jnp.bfloat16),
            pltpu.VMEM((1, width), jnp.float32),
            pltpu.VMEM((1, HEAD_SIZE), jnp.float32),
        ),
        cost(2 * source_rows * width * 512, 3000000),
        [HBM] * 8,
        (VMEM, VMEM, HBM, VMEM, VMEM),
        (
            pltpu.VMEM((own_rows, width), jnp.bfloat16),
            pltpu.VMEM((source_rows, width), jnp.bfloat16),
            pltpu.VMEM((1, width), jnp.float32),
            pltpu.VMEM((KEY_VALUE_HEADS, HEAD_SIZE), jnp.float32),
            pltpu.VMEM((4, depth, 2 * HEAD_SIZE), jnp.bfloat16),
            pltpu.VMEM((4, depth, 2 * HEAD_SIZE), jnp.bfloat16),
            pltpu.SemaphoreType.DMA((6,)),
            pltpu.SemaphoreType.DMA((4, 2)),
            pltpu.SemaphoreType.DMA((tp,)),
        ),
        vmem=16 * 1024 * 1024,
    )(
        *(
            pltpu.with_memory_space_constraint(x, pltpu.HBM)
            for x in (
                target,
                source,
                source_gain.reshape(1, width),
                key_matrix,
                value_matrix,
                key_gain,
                target_gain.reshape(1, width),
                query_gain,
            )
        )
    )
    received = lax.ppermute(other, "tp", opposite)
    everyone = lax.all_to_all(target_copies, "tp", 0, 0, tiled=True)
    everyone = everyone.reshape(block, width)
    near = lax.all_gather(
        jnp.concatenate([own, received], axis=0),
        "sp",
        axis=0,
        tiled=True,
        axis_index_groups=along_z,
    )
    copies = call(
        query_kernel,
        pltpu.HBM((GROUP, block, HEAD_SIZE), jnp.bfloat16),
        cost(2 * block * width * HEAD_SIZE, 1400000),
        [VMEM] * 4,
        HBM,
        (
            pltpu.VMEM((block, HEAD_SIZE), jnp.bfloat16),
            pltpu.SemaphoreType.DMA((GROUP,)),
        ),
    )(everyone, target_gain_here, query_weight, query_gain_here)
    all_queries = lax.all_to_all(
        copies, "tp", 0, 0, tiled=True, axis_index_groups=halves
    )
    far = lax.ppermute(near, "sp", [(i, i ^ 1) for i in range(sp)])
    pair_weight = lax.ppermute(out_weight, "tp", [(i, i ^ 2) for i in range(tp)])
    keys = 2 * near.shape[0]
    partials = call(
        attention_kernel,
        pltpu.HBM((GROUP, block + STAT_ROWS, HEAD_SIZE), jnp.bfloat16),
        cost(4 * GROUP * block * keys * HEAD_SIZE, 2500000, GROUP * block * keys),
        [VMEM] * 3,
        HBM,
        (
            pltpu.VMEM((GROUP, block + STAT_ROWS, HEAD_SIZE), jnp.bfloat16),
            pltpu.SemaphoreType.DMA((GROUP,)),
        ),
    )(all_queries, near, far)
    mine = lax.all_to_all(partials, "tp", 0, 0, tiled=True, axis_index_groups=halves)
    update = call(
        output_kernel,
        bf16(tp // 2, own_rows, width),
        cost(2 * block * width * HEAD_SIZE, 1900000),
        [VMEM] * 3,
    )(mine, out_weight, pair_weight)
    parts = lax.all_to_all(update, "tp", 0, 0, tiled=True, axis_index_groups=sides)
    return call(
        final_kernel,
        bf16(own_rows, width),
        cost(tp // 2 * own_rows * width, 300000),
        [VMEM] * 2,
    )(target, parts)


def solution(mesh):
    return jax.shard_map(
        body,
        mesh=mesh,
        in_specs=(
            P(("sp", "tp"), None),
            P(("sp", "tp"), None),
            P(),
            P(),
            P(None, "tp"),
            P(),
            P(),
            P("tp", None),
            P(),
            P("tp", None),
        ),
        out_specs=P(("sp", "tp"), None),
        check_vma=False,
    )
```

```python
import math

import jax
import jax.numpy as jnp
from jax import lax
from jax.experimental import pallas as pl
from jax.experimental.pallas import tpu as pltpu
from jax.sharding import PartitionSpec as P


QUERY_HEAD_COUNT = 16
KEY_VALUE_HEADS = 2
HEAD_SIZE = 128
GROUP = QUERY_HEAD_COUNT // KEY_VALUE_HEADS
EPSILON = 1e-06
EXP2_SCALE = math.log2(math.e) / math.sqrt(HEAD_SIZE)
STAT_ROWS = 16

VMEM = pl.BlockSpec(memory_space=pltpu.VMEM)
HBM = pl.BlockSpec(memory_space=pltpu.HBM)


def cost(flops, nbytes, transcendentals=0):
    return pl.CostEstimate(
        flops=flops, bytes_accessed=nbytes, transcendentals=transcendentals
    )


def normed(values_in, gain):
    return (
        values_in
        * lax.rsqrt(jnp.mean(values_in * values_in, axis=-1, keepdims=True) + EPSILON)
        * gain
    )


def key_value_kernel(
    target,
    source,
    gain,
    key_matrix,
    value_matrix,
    key_gain,
    target_gain,
    query_gain,
    own,
    other,
    target_copies,
    target_gain_here,
    query_gain_here,
    target_here,
    source_here,
    gain_here,
    key_gain_here,
    key_part,
    value_part,
    arrived,
    matrix_arrived,
    left,
):
    depth = key_part.shape[1]
    parts = key_part.shape[0]
    inputs = [
        pltpu.make_async_copy(a, b, arrived.at[i])
        for i, (a, b) in enumerate(
            (
                (target, target_here),
                (source, source_here),
                (gain, gain_here),
                (key_gain, key_gain_here),
                (target_gain, target_gain_here),
                (query_gain, query_gain_here),
            )
        )
    ]
    matrices = [
        pltpu.make_async_copy(
            matrix.at[pl.ds(i * depth, depth), :], buffer.at[i], matrix_arrived.at[i, j]
        )
        for i in range(parts)
        for j, (matrix, buffer) in enumerate(
            ((key_matrix, key_part), (value_matrix, value_part))
        )
    ]
    outputs = [
        pltpu.make_async_copy(target_here, target_copies.at[i], left.at[i])
        for i in range(target_copies.shape[0])
    ]
    for c in inputs + matrices:
        c.start()
    inputs[0].wait()
    for c in outputs:
        c.start()
    second = lax.axis_index("tp") >= GROUP
    for c in inputs[1:]:
        c.wait()
    rows = normed(source_here[...].astype(jnp.float32), gain_here[...])
    rows = rows.astype(jnp.bfloat16)
    raw, values = 0.0, 0.0
    for i in range(parts):
        matrices[2 * i].wait()
        matrices[2 * i + 1].wait()
        part = rows[:, i * depth : (i + 1) * depth]
        raw += jnp.dot(part, key_part[i], preferred_element_type=jnp.float32)
        values += jnp.dot(part, value_part[i], preferred_element_type=jnp.float32)
    values = values.astype(jnp.bfloat16)
    heads = []
    for h in range(KEY_VALUE_HEADS):
        at = slice(h * HEAD_SIZE, (h + 1) * HEAD_SIZE)
        keys = normed(raw[:, at], key_gain_here[h : h + 1, :]).astype(jnp.bfloat16)
        heads.append(jnp.concatenate([keys, values[:, at]], axis=1))
    own[...] = jnp.where(second, heads[1], heads[0])
    other[...] = jnp.where(second, heads[0], heads[1])
    for c in outputs:
        c.wait()


def query_kernel(target, gain, weight, head_gain, copies, here, left):
    rows = normed(target[...].astype(jnp.float32), gain[...]).astype(jnp.bfloat16)
    raw = jnp.dot(rows, weight[...], preferred_element_type=jnp.float32)
    here[...] = normed(raw, head_gain[...]).astype(jnp.bfloat16)
    outputs = [
        pltpu.make_async_copy(here, copies.at[i], left.at[i]) for i in range(GROUP)
    ]
    for c in outputs:
        c.start()
    for c in outputs:
        c.wait()


def in_three(x):
    first = x.astype(jnp.bfloat16)
    rest = x - first.astype(jnp.float32)
    second = rest.astype(jnp.bfloat16)
    third = (rest - second.astype(jnp.float32)).astype(jnp.bfloat16)
    return [first, second, third]


def attention_kernel(queries, near, far, out):
    rows = GROUP * HEAD_SIZE
    at_row = lax.broadcasted_iota(jnp.int32, (HEAD_SIZE, HEAD_SIZE), 0)
    at_lane = lax.broadcasted_iota(jnp.int32, (HEAD_SIZE, HEAD_SIZE), 1)
    eye = (at_row == at_lane).astype(jnp.float32)
    q = queries[...].reshape(rows, HEAD_SIZE)
    peak = None
    for kv in (near, far):
        scores = lax.dot_general(
            q,
            kv[:, :HEAD_SIZE],
            (((1,), (1,)), ((), ())),
            preferred_element_type=jnp.float32,
        )
        highest = jnp.max(scores, axis=-1, keepdims=True)
        before, peak = peak, highest if peak is None else jnp.maximum(peak, highest)
        weights = jnp.exp2((scores - peak) * EXP2_SCALE)
        share = jnp.sum(weights, axis=-1, keepdims=True)
        part = jnp.dot(
            weights.astype(jnp.bfloat16),
            kv[:, HEAD_SIZE:],
            preferred_element_type=jnp.float32,
        )
        if before is None:
            total, weighted = share, part
        else:
            fade = jnp.exp2((before - peak) * EXP2_SCALE)
            total, weighted = total * fade + share, weighted * fade + part

    def as_rows(column, head):
        at = slice(head * HEAD_SIZE, (head + 1) * HEAD_SIZE)
        return in_three(jnp.sum(eye * column[at], axis=0, keepdims=True))

    for head in range(GROUP):
        if head % 4 >= 2:
            continue
        stats = []
        for h in (head, head + 2):
            stats += as_rows(peak, h) + as_rows(total, h)
        empty = jnp.zeros((STAT_ROWS - len(stats), HEAD_SIZE), jnp.bfloat16)
        stats = jnp.concatenate(stats + [empty], axis=0)
        for side in range(2):
            to = head + 2 * side
            out[to, :HEAD_SIZE, :] = jnp.concatenate(
                [
                    weighted[h * HEAD_SIZE + i : h * HEAD_SIZE + i + 16]
                    for h in (head, head + 2)
                    for i in range(16 * side, HEAD_SIZE, 32)
                ],
                axis=0,
            ).astype(jnp.bfloat16)
            out[to, HEAD_SIZE:, :] = stats


def combine_kernel(partials, own, pair):
    is_high = lax.rem(lax.axis_index("tp"), 4) >= 2
    half = HEAD_SIZE // 2
    row = lax.broadcasted_iota(jnp.int32, (half, HEAD_SIZE), 0)
    lane = lax.broadcasted_iota(jnp.int32, (half, HEAD_SIZE), 1)
    place = row + (row // 16) * 16 + jnp.where(is_high, 16, 0)
    selection = (lane == place).astype(jnp.float32)
    stats = [partials[j, HEAD_SIZE:, :].astype(jnp.float32) for j in range(GROUP)]
    results = []
    for k in range(2):
        peaks = [s[6 * k : 6 * k + 1] + s[6 * k + 1 : 6 * k + 2] + s[6 * k + 2 : 6 * k + 3] for s in stats]
        totals = [s[6 * k + 3 : 6 * k + 4] + s[6 * k + 4 : 6 * k + 5] + s[6 * k + 5 : 6 * k + 6] for s in stats]
        peak = peaks[0]
        for p in peaks[1:]:
            peak = jnp.maximum(peak, p)
        fades = [jnp.exp2((p - peak) * EXP2_SCALE) for p in peaks]
        total = fades[0] * totals[0]
        for f, t in zip(fades[1:], totals[1:]):
            total += f * t
        attended = 0.0
        for j in range(GROUP):
            column = jnp.sum(selection * (fades[j] / total), axis=1, keepdims=True)
            attended += column * partials[j, half * k : half * (k + 1), :].astype(jnp.float32)
        results.append(attended.astype(jnp.bfloat16))
    low, high = results
    own[...] = jnp.where(is_high, high, low)
    pair[...] = jnp.where(is_high, low, high)


def output_kernel(own, pair, own_weight, pair_weight, out):
    update = jnp.dot(own[...], own_weight[...], preferred_element_type=jnp.float32)
    update += jnp.dot(pair[...], pair_weight[...], preferred_element_type=jnp.float32)
    out[...] = update.astype(jnp.bfloat16).reshape(out.shape)


def final_kernel(target, parts, out):
    update = parts[0].astype(jnp.float32)
    for i in range(1, parts.shape[0]):
        update += parts[i].astype(jnp.float32)
    out[...] = (target[...].astype(jnp.float32) + update).astype(jnp.bfloat16)


def call(kernel, outs, estimate, specs, out_specs=None, scratch=(), vmem=32 * 1024 * 1024):
    return pl.pallas_call(
        kernel,
        out_shape=outs,
        in_specs=specs,
        scratch_shapes=list(scratch),
        out_specs=out_specs or jax.tree.map(lambda _: VMEM, outs),
        cost_estimate=estimate,
        compiler_params=pltpu.CompilerParams(vmem_limit_bytes=vmem),
    )


def bf16(*shape):
    return jax.ShapeDtypeStruct(shape, jnp.bfloat16)


def body(
    target,
    source,
    target_gain,
    source_gain,
    query_weight,
    key_matrix,
    value_matrix,
    query_gain,
    key_gain,
    out_weight,
):
    width = target.shape[1]
    tp = lax.axis_size("tp")
    sp = lax.axis_size("sp")
    own_rows = target.shape[0]
    block = own_rows * tp
    source_rows = source.shape[0]
    halves = [[i + h * GROUP for i in range(GROUP)] for h in range(KEY_VALUE_HEADS)]
    sides = [[i for i in range(tp) if i // 2 % 2 == e] for e in range(2)]
    along_z = [[2 * z + (z + core) % 2 for z in range(sp // 2)] for core in range(2)]
    side = math.isqrt(tp)
    opposite = [(i, (side - 1 - i // side) * side + i % side) for i in range(tp)]
    depth = width // 4

    pieces = (source_rows, 2 * HEAD_SIZE)
    own, other, target_copies, target_gain_here, query_gain_here = call(
        key_value_kernel,
        (
            pltpu.VMEM(pieces, jnp.bfloat16),
            pltpu.VMEM(pieces, jnp.bfloat16),
            pltpu.HBM((tp, own_rows, width), jnp.bfloat16),
            pltpu.VMEM((1, width), jnp.float32),
            pltpu.VMEM((1, HEAD_SIZE), jnp.float32),
        ),
        cost(2 * source_rows * width * 512, 3000000),
        [HBM] * 8,
        (VMEM, VMEM, HBM, VMEM, VMEM),
        (
            pltpu.VMEM((own_rows, width), jnp.bfloat16),
            pltpu.VMEM((source_rows, width), jnp.bfloat16),
            pltpu.VMEM((1, width), jnp.float32),
            pltpu.VMEM((KEY_VALUE_HEADS, HEAD_SIZE), jnp.float32),
            pltpu.VMEM((4, depth, 2 * HEAD_SIZE), jnp.bfloat16),
            pltpu.VMEM((4, depth, 2 * HEAD_SIZE), jnp.bfloat16),
            pltpu.SemaphoreType.DMA((6,)),
            pltpu.SemaphoreType.DMA((4, 2)),
            pltpu.SemaphoreType.DMA((tp,)),
        ),
        vmem=16 * 1024 * 1024,
    )(
        *(
            pltpu.with_memory_space_constraint(x, pltpu.HBM)
            for x in (
                target,
                source,
                source_gain.reshape(1, width),
                key_matrix,
                value_matrix,
                key_gain,
                target_gain.reshape(1, width),
                query_gain,
            )
        )
    )
    received = lax.ppermute(other, "tp", opposite)
    everyone = lax.all_to_all(target_copies, "tp", 0, 0, tiled=True)
    everyone = everyone.reshape(block, width)
    near = lax.all_gather(
        jnp.concatenate([own, received], axis=0),
        "sp",
        axis=0,
        tiled=True,
        axis_index_groups=along_z,
    )
    copies = call(
        query_kernel,
        pltpu.HBM((GROUP, block, HEAD_SIZE), jnp.bfloat16),
        cost(2 * block * width * HEAD_SIZE, 1400000),
        [VMEM] * 4,
        HBM,
        (
            pltpu.VMEM((block, HEAD_SIZE), jnp.bfloat16),
            pltpu.SemaphoreType.DMA((GROUP,)),
        ),
    )(everyone, target_gain_here, query_weight, query_gain_here)
    all_queries = lax.all_to_all(
        copies, "tp", 0, 0, tiled=True, axis_index_groups=halves
    )
    far = lax.ppermute(near, "sp", [(i, i ^ 1) for i in range(sp)])
    pair_weight = lax.ppermute(out_weight, "tp", [(i, i ^ 2) for i in range(tp)])
    keys = 2 * near.shape[0]
    partials = call(
        attention_kernel,
        bf16(GROUP, block + STAT_ROWS, HEAD_SIZE),
        cost(4 * GROUP * block * keys * HEAD_SIZE, 2500000, GROUP * block * keys),
        [VMEM] * 3,
    )(all_queries, near, pltpu.with_memory_space_constraint(far, pltpu.VMEM))
    mine = lax.all_to_all(partials, "tp", 0, 0, tiled=True, axis_index_groups=halves)
    half = bf16(block // 2, HEAD_SIZE)
    own_part, pair_part = call(
        combine_kernel, (half, half), cost(4 * GROUP * block * HEAD_SIZE, 400000), [VMEM]
    )(mine)
    update = call(
        output_kernel,
        bf16(tp // 2, own_rows, width),
        cost(2 * block * width * HEAD_SIZE, 1900000),
        [VMEM] * 4,
    )(own_part, pair_part, out_weight, pair_weight)
    parts = lax.all_to_all(update, "tp", 0, 0, tiled=True, axis_index_groups=sides)
    return call(
        final_kernel,
        bf16(own_rows, width),
        cost(tp // 2 * own_rows * width, 300000),
        [VMEM] * 2,
    )(target, parts)


def solution(mesh):
    return jax.shard_map(
        body,
        mesh=mesh,
        in_specs=(
            P(("sp", "tp"), None),
            P(("sp", "tp"), None),
            P(),
            P(),
            P(None, "tp"),
            P(),
            P(),
            P("tp", None),
            P(),
            P("tp", None),
        ),
        out_specs=P(("sp", "tp"), None),
        check_vma=False,
    )
```

```python
import math

import jax
import jax.numpy as jnp
from jax import lax
from jax.experimental import pallas as pl
from jax.experimental.pallas import tpu as pltpu
from jax.sharding import PartitionSpec as P


QUERY_HEAD_COUNT = 16
KEY_VALUE_HEADS = 2
HEAD_SIZE = 128
GROUP = QUERY_HEAD_COUNT // KEY_VALUE_HEADS
EPSILON = 1e-06
EXP2_SCALE = math.log2(math.e) / math.sqrt(HEAD_SIZE)
STAT_ROWS = 16

VMEM = pl.BlockSpec(memory_space=pltpu.VMEM)
HBM = pl.BlockSpec(memory_space=pltpu.HBM)


def cost(flops, nbytes, transcendentals=0):
    return pl.CostEstimate(
        flops=flops, bytes_accessed=nbytes, transcendentals=transcendentals
    )


def normed(values_in, gain):
    return (
        values_in
        * lax.rsqrt(jnp.mean(values_in * values_in, axis=-1, keepdims=True) + EPSILON)
        * gain
    )


def key_value_kernel(
    target,
    source,
    gain,
    key_matrix,
    value_matrix,
    key_gain,
    target_gain,
    query_gain,
    own,
    other,
    target_copies,
    target_gain_here,
    query_gain_here,
    target_here,
    source_here,
    gain_here,
    key_gain_here,
    key_part,
    value_part,
    arrived,
    matrix_arrived,
    left,
):
    depth = key_part.shape[1]
    parts = key_part.shape[0]
    inputs = [
        pltpu.make_async_copy(a, b, arrived.at[i])
        for i, (a, b) in enumerate(
            (
                (target, target_here),
                (source, source_here),
                (gain, gain_here),
                (key_gain, key_gain_here),
                (target_gain, target_gain_here),
                (query_gain, query_gain_here),
            )
        )
    ]
    matrices = [
        pltpu.make_async_copy(
            matrix.at[pl.ds(i * depth, depth), :], buffer.at[i], matrix_arrived.at[i, j]
        )
        for i in range(parts)
        for j, (matrix, buffer) in enumerate(
            ((key_matrix, key_part), (value_matrix, value_part))
        )
    ]
    outputs = [
        pltpu.make_async_copy(target_here, target_copies.at[i], left.at[i])
        for i in range(target_copies.shape[0])
    ]
    for c in inputs + matrices:
        c.start()
    inputs[0].wait()
    for c in outputs:
        c.start()
    second = lax.axis_index("tp") >= GROUP
    for c in inputs[1:]:
        c.wait()
    rows = normed(source_here[...].astype(jnp.float32), gain_here[...])
    rows = rows.astype(jnp.bfloat16)
    raw, values = 0.0, 0.0
    for i in range(parts):
        matrices[2 * i].wait()
        matrices[2 * i + 1].wait()
        part = rows[:, i * depth : (i + 1) * depth]
        raw += jnp.dot(part, key_part[i], preferred_element_type=jnp.float32)
        values += jnp.dot(part, value_part[i], preferred_element_type=jnp.float32)
    values = values.astype(jnp.bfloat16)
    heads = []
    for h in range(KEY_VALUE_HEADS):
        at = slice(h * HEAD_SIZE, (h + 1) * HEAD_SIZE)
        keys = normed(raw[:, at], key_gain_here[h : h + 1, :]).astype(jnp.bfloat16)
        heads.append(jnp.concatenate([keys, values[:, at]], axis=1))
    own[...] = jnp.where(second, heads[1], heads[0])
    other[...] = jnp.where(second, heads[0], heads[1])
    for c in outputs:
        c.wait()


def query_kernel(target, gain, weight, head_gain, copies, here, left):
    rows = normed(target[...].astype(jnp.float32), gain[...]).astype(jnp.bfloat16)
    raw = jnp.dot(rows, weight[...], preferred_element_type=jnp.float32)
    here[...] = normed(raw, head_gain[...]).astype(jnp.bfloat16)
    outputs = [
        pltpu.make_async_copy(here, copies.at[i], left.at[i]) for i in range(GROUP)
    ]
    for c in outputs:
        c.start()
    for c in outputs:
        c.wait()


def in_three(x):
    first = x.astype(jnp.bfloat16)
    rest = x - first.astype(jnp.float32)
    second = rest.astype(jnp.bfloat16)
    third = (rest - second.astype(jnp.float32)).astype(jnp.bfloat16)
    return [first, second, third]


def is_inner(device):
    return device % 4 in (1, 2)


def attention_kernel(queries, near, far, out):
    rows = GROUP * HEAD_SIZE
    at_row = lax.broadcasted_iota(jnp.int32, (HEAD_SIZE, HEAD_SIZE), 0)
    at_lane = lax.broadcasted_iota(jnp.int32, (HEAD_SIZE, HEAD_SIZE), 1)
    eye = (at_row == at_lane).astype(jnp.float32)
    q = queries[...].reshape(rows, HEAD_SIZE)
    peak = None
    for kv in (near, far):
        scores = lax.dot_general(
            q,
            kv[:, :HEAD_SIZE],
            (((1,), (1,)), ((), ())),
            preferred_element_type=jnp.float32,
        )
        highest = jnp.max(scores, axis=-1, keepdims=True)
        before, peak = peak, highest if peak is None else jnp.maximum(peak, highest)
        weights = jnp.exp2((scores - peak) * EXP2_SCALE)
        share = jnp.sum(weights, axis=-1, keepdims=True)
        part = jnp.dot(
            weights.astype(jnp.bfloat16),
            kv[:, HEAD_SIZE:],
            preferred_element_type=jnp.float32,
        )
        if before is None:
            total, weighted = share, part
        else:
            fade = jnp.exp2((before - peak) * EXP2_SCALE)
            total, weighted = total * fade + share, weighted * fade + part

    def as_rows(column, head):
        at = slice(head * HEAD_SIZE, (head + 1) * HEAD_SIZE)
        return in_three(jnp.sum(eye * column[at], axis=0, keepdims=True))

    for head in range(0, GROUP, 2):
        stats = []
        for h in (head, head + 1):
            stats += as_rows(peak, h) + as_rows(total, h)
        empty = jnp.zeros((STAT_ROWS - len(stats), HEAD_SIZE), jnp.bfloat16)
        stats = jnp.concatenate(stats + [empty], axis=0)
        for h in (head, head + 1):
            starts = (8, 16) if is_inner(h) else (0, 24)
            out[h, :HEAD_SIZE, :] = jnp.concatenate(
                [
                    weighted[i + start : i + start + 8]
                    for i in range(head * HEAD_SIZE, (head + 2) * HEAD_SIZE, 32)
                    for start in starts
                ],
                axis=0,
            ).astype(jnp.bfloat16)
            out[h, HEAD_SIZE:, :] = stats


def combine_kernel(partials, own, pair):
    x = lax.rem(lax.axis_index("tp"), 4)
    is_high = lax.rem(x, 2) == 1
    inner = (x == 1) | (x == 2)
    half = HEAD_SIZE // 2
    row = lax.broadcasted_iota(jnp.int32, (half, HEAD_SIZE), 0)
    lane = lax.broadcasted_iota(jnp.int32, (half, HEAD_SIZE), 1)
    outer_place = jnp.where(row % 16 >= 8, 16, 0)
    place = row + (row // 16) * 16 + jnp.where(inner, 8, outer_place)
    selection = (lane == place).astype(jnp.float32)
    stats = [partials[j, HEAD_SIZE:, :].astype(jnp.float32) for j in range(GROUP)]
    results = []
    for k in range(2):
        peaks = [s[6 * k : 6 * k + 1] + s[6 * k + 1 : 6 * k + 2] + s[6 * k + 2 : 6 * k + 3] for s in stats]
        totals = [s[6 * k + 3 : 6 * k + 4] + s[6 * k + 4 : 6 * k + 5] + s[6 * k + 5 : 6 * k + 6] for s in stats]
        peak = peaks[0]
        for p in peaks[1:]:
            peak = jnp.maximum(peak, p)
        fades = [jnp.exp2((p - peak) * EXP2_SCALE) for p in peaks]
        total = fades[0] * totals[0]
        for f, t in zip(fades[1:], totals[1:]):
            total += f * t
        attended = 0.0
        for j in range(GROUP):
            column = jnp.sum(selection * (fades[j] / total), axis=1, keepdims=True)
            attended += column * partials[j, half * k : half * (k + 1), :].astype(jnp.float32)
        results.append(attended.astype(jnp.bfloat16))
    low, high = results
    own[...] = jnp.where(is_high, high, low)
    pair[...] = jnp.where(is_high, low, high)


def output_kernel(own, pair, own_weight, pair_weight, out):
    update = jnp.dot(own[...], own_weight[...], preferred_element_type=jnp.float32)
    update += jnp.dot(pair[...], pair_weight[...], preferred_element_type=jnp.float32)
    out[...] = update.astype(jnp.bfloat16).reshape(out.shape)


def final_kernel(target, parts, out):
    update = parts[0].astype(jnp.float32)
    for i in range(1, parts.shape[0]):
        update += parts[i].astype(jnp.float32)
    out[...] = (target[...].astype(jnp.float32) + update).astype(jnp.bfloat16)


def call(kernel, outs, estimate, specs, out_specs=None, scratch=(), vmem=48 * 1024 * 1024):
    return pl.pallas_call(
        kernel,
        out_shape=outs,
        in_specs=specs,
        scratch_shapes=list(scratch),
        out_specs=out_specs or jax.tree.map(lambda _: VMEM, outs),
        cost_estimate=estimate,
        compiler_params=pltpu.CompilerParams(vmem_limit_bytes=vmem),
    )


def bf16(*shape):
    return jax.ShapeDtypeStruct(shape, jnp.bfloat16)


def body(
    target,
    source,
    target_gain,
    source_gain,
    query_weight,
    key_matrix,
    value_matrix,
    query_gain,
    key_gain,
    out_weight,
):
    width = target.shape[1]
    tp = lax.axis_size("tp")
    sp = lax.axis_size("sp")
    own_rows = target.shape[0]
    block = own_rows * tp
    source_rows = source.shape[0]
    halves = [[i + h * GROUP for i in range(GROUP)] for h in range(KEY_VALUE_HEADS)]
    sides = [[i for i in range(tp) if is_inner(i) == e] for e in (False, True)]
    along_z = [[2 * z + (z + core) % 2 for z in range(sp // 2)] for core in range(2)]
    side = math.isqrt(tp)
    opposite = [(i, (side - 1 - i // side) * side + i % side) for i in range(tp)]
    depth = width // 4

    pieces = (source_rows, 2 * HEAD_SIZE)
    own, other, target_copies, target_gain_here, query_gain_here = call(
        key_value_kernel,
        (
            pltpu.VMEM(pieces, jnp.bfloat16),
            pltpu.VMEM(pieces, jnp.bfloat16),
            pltpu.HBM((tp, own_rows, width), jnp.bfloat16),
            pltpu.VMEM((1, width), jnp.float32),
            pltpu.VMEM((1, HEAD_SIZE), jnp.float32),
        ),
        cost(2 * source_rows * width * 512, 3000000),
        [HBM] * 8,
        (VMEM, VMEM, HBM, VMEM, VMEM),
        (
            pltpu.VMEM((own_rows, width), jnp.bfloat16),
            pltpu.VMEM((source_rows, width), jnp.bfloat16),
            pltpu.VMEM((1, width), jnp.float32),
            pltpu.VMEM((KEY_VALUE_HEADS, HEAD_SIZE), jnp.float32),
            pltpu.VMEM((4, depth, 2 * HEAD_SIZE), jnp.bfloat16),
            pltpu.VMEM((4, depth, 2 * HEAD_SIZE), jnp.bfloat16),
            pltpu.SemaphoreType.DMA((6,)),
            pltpu.SemaphoreType.DMA((4, 2)),
            pltpu.SemaphoreType.DMA((tp,)),
        ),
        vmem=16 * 1024 * 1024,
    )(
        *(
            pltpu.with_memory_space_constraint(x, pltpu.HBM)
            for x in (
                target,
                source,
                source_gain.reshape(1, width),
                key_matrix,
                value_matrix,
                key_gain,
                target_gain.reshape(1, width),
                query_gain,
            )
        )
    )
    received = lax.ppermute(other, "tp", opposite)
    everyone = lax.all_to_all(target_copies, "tp", 0, 0, tiled=True)
    everyone = everyone.reshape(block, width)
    near = lax.all_gather(
        jnp.concatenate([own, received], axis=0),
        "sp",
        axis=0,
        tiled=True,
        axis_index_groups=along_z,
    )
    copies = call(
        query_kernel,
        pltpu.HBM((GROUP, block, HEAD_SIZE), jnp.bfloat16),
        cost(2 * block * width * HEAD_SIZE, 1400000),
        [VMEM] * 4,
        HBM,
        (
            pltpu.VMEM((block, HEAD_SIZE), jnp.bfloat16),
            pltpu.SemaphoreType.DMA((GROUP,)),
        ),
    )(everyone, target_gain_here, query_weight, query_gain_here)
    all_queries = lax.all_to_all(
        copies, "tp", 0, 0, tiled=True, axis_index_groups=halves
    )
    far = lax.ppermute(near, "sp", [(i, i ^ 1) for i in range(sp)])
    pair_weight = lax.ppermute(out_weight, "tp", [(i, i ^ 1) for i in range(tp)])
    keys = 2 * near.shape[0]
    partials = call(
        attention_kernel,
        bf16(GROUP, block + STAT_ROWS, HEAD_SIZE),
        cost(4 * GROUP * block * keys * HEAD_SIZE, 2500000, GROUP * block * keys),
        [VMEM] * 3,
    )(all_queries, near, far)
    mine = lax.all_to_all(partials, "tp", 0, 0, tiled=True, axis_index_groups=halves)
    half = bf16(block // 2, HEAD_SIZE)
    own_part, pair_part = call(
        combine_kernel, (half, half), cost(4 * GROUP * block * HEAD_SIZE, 400000), [VMEM]
    )(mine)
    update = call(
        output_kernel,
        bf16(tp // 2, own_rows, width),
        cost(2 * block * width * HEAD_SIZE, 1900000),
        [VMEM] * 4,
    )(own_part, pair_part, out_weight, pair_weight)
    parts = lax.all_to_all(update, "tp", 0, 0, tiled=True, axis_index_groups=sides)
    return call(
        final_kernel,
        bf16(own_rows, width),
        cost(tp // 2 * own_rows * width, 300000),
        [VMEM] * 2,
    )(target, parts)


def solution(mesh):
    return jax.shard_map(
        body,
        mesh=mesh,
        in_specs=(
            P(("sp", "tp"), None),
            P(("sp", "tp"), None),
            P(),
            P(),
            P(None, "tp"),
            P(),
            P(),
            P("tp", None),
            P(),
            P("tp", None),
        ),
        out_specs=P(("sp", "tp"), None),
        check_vma=False,
    )
```

```python
import math

import jax
import jax.numpy as jnp
from jax import lax
from jax.experimental import pallas as pl
from jax.experimental.pallas import tpu as pltpu
from jax.sharding import PartitionSpec as P


QUERY_HEAD_COUNT = 16
KEY_VALUE_HEADS = 2
HEAD_SIZE = 128
GROUP = QUERY_HEAD_COUNT // KEY_VALUE_HEADS
EPSILON = 1e-06
EXP2_SCALE = math.log2(math.e) / math.sqrt(HEAD_SIZE)
STAT_ROWS = 16

VMEM = pl.BlockSpec(memory_space=pltpu.VMEM)
HBM = pl.BlockSpec(memory_space=pltpu.HBM)


def cost(flops, nbytes, transcendentals=0):
    return pl.CostEstimate(
        flops=flops, bytes_accessed=nbytes, transcendentals=transcendentals
    )


def normed(values_in, gain):
    return (
        values_in
        * lax.rsqrt(jnp.mean(values_in * values_in, axis=-1, keepdims=True) + EPSILON)
        * gain
    )


def key_value_kernel(
    target,
    source,
    gain,
    key_matrix,
    value_matrix,
    key_gain,
    target_gain,
    query_gain,
    own,
    other,
    target_copies,
    target_gain_here,
    query_gain_here,
    target_here,
    source_here,
    gain_here,
    key_gain_here,
    key_part,
    value_part,
    arrived,
    matrix_arrived,
    left,
):
    depth = key_part.shape[1]
    parts = key_part.shape[0]
    inputs = [
        pltpu.make_async_copy(a, b, arrived.at[i])
        for i, (a, b) in enumerate(
            (
                (target, target_here),
                (source, source_here),
                (gain, gain_here),
                (key_gain, key_gain_here),
                (target_gain, target_gain_here),
                (query_gain, query_gain_here),
            )
        )
    ]
    matrices = [
        pltpu.make_async_copy(
            matrix.at[pl.ds(i * depth, depth), :], buffer.at[i], matrix_arrived.at[i, j]
        )
        for i in range(parts)
        for j, (matrix, buffer) in enumerate(
            ((key_matrix, key_part), (value_matrix, value_part))
        )
    ]
    outputs = [
        pltpu.make_async_copy(target_here, target_copies.at[i], left.at[i])
        for i in range(target_copies.shape[0])
    ]
    for c in inputs + matrices:
        c.start()
    inputs[0].wait()
    for c in outputs:
        c.start()
    second = lax.axis_index("tp") >= GROUP
    for c in inputs[1:]:
        c.wait()
    rows = normed(source_here[...].astype(jnp.float32), gain_here[...])
    rows = rows.astype(jnp.bfloat16)
    raw, values = 0.0, 0.0
    for i in range(parts):
        matrices[2 * i].wait()
        matrices[2 * i + 1].wait()
        part = rows[:, i * depth : (i + 1) * depth]
        raw += jnp.dot(part, key_part[i], preferred_element_type=jnp.float32)
        values += jnp.dot(part, value_part[i], preferred_element_type=jnp.float32)
    values = values.astype(jnp.bfloat16)
    heads = []
    for h in range(KEY_VALUE_HEADS):
        at = slice(h * HEAD_SIZE, (h + 1) * HEAD_SIZE)
        keys = normed(raw[:, at], key_gain_here[h : h + 1, :]).astype(jnp.bfloat16)
        heads.append(jnp.concatenate([keys, values[:, at]], axis=1))
    own[...] = jnp.where(second, heads[1], heads[0])
    other[...] = jnp.where(second, heads[0], heads[1])
    for c in outputs:
        c.wait()


def query_kernel(target, gain, weight, head_gain, copies, here, left):
    rows = normed(target[...].astype(jnp.float32), gain[...]).astype(jnp.bfloat16)
    raw = jnp.dot(rows, weight[...], preferred_element_type=jnp.float32)
    here[...] = normed(raw, head_gain[...]).astype(jnp.bfloat16)
    outputs = [
        pltpu.make_async_copy(here, copies.at[i], left.at[i]) for i in range(GROUP)
    ]
    for c in outputs:
        c.start()
    for c in outputs:
        c.wait()


def in_three(x):
    first = x.astype(jnp.bfloat16)
    rest = x - first.astype(jnp.float32)
    second = rest.astype(jnp.bfloat16)
    third = (rest - second.astype(jnp.float32)).astype(jnp.bfloat16)
    return [first, second, third]


def attended_part(queries, kv, before=None):
    scores = lax.dot_general(
        queries[...].reshape(GROUP * HEAD_SIZE, HEAD_SIZE),
        kv[:, :HEAD_SIZE],
        (((1,), (1,)), ((), ())),
        preferred_element_type=jnp.float32,
    )
    peak = jnp.max(scores, axis=-1, keepdims=True)
    if before is not None:
        peak = jnp.maximum(before, peak)
    weights = jnp.exp2((scores - peak) * EXP2_SCALE)
    total = jnp.sum(weights, axis=-1, keepdims=True)
    weighted = jnp.dot(
        weights.astype(jnp.bfloat16), kv[:, HEAD_SIZE:], preferred_element_type=jnp.float32
    )
    return peak, total, weighted


def near_kernel(queries, kv, peaks, totals, sums):
    peak, total, weighted = attended_part(queries, kv)
    peaks[...] = jnp.broadcast_to(peak, peaks.shape)
    totals[...] = jnp.broadcast_to(total, totals.shape)
    sums[...] = weighted


def far_kernel(queries, kv, peaks, totals, sums, out):
    at_row = lax.broadcasted_iota(jnp.int32, (HEAD_SIZE, HEAD_SIZE), 0)
    at_lane = lax.broadcasted_iota(jnp.int32, (HEAD_SIZE, HEAD_SIZE), 1)
    eye = (at_row == at_lane).astype(jnp.float32)
    before = peaks[:, :1]
    peak, share, part = attended_part(queries, kv, before)
    fade = jnp.exp2((before - peak) * EXP2_SCALE)
    total = totals[:, :1] * fade + share
    weighted = sums[...] * fade + part

    def as_rows(column, head):
        at = slice(head * HEAD_SIZE, (head + 1) * HEAD_SIZE)
        return in_three(jnp.sum(eye * column[at], axis=0, keepdims=True))

    for head in range(GROUP):
        if head % 4 >= 2:
            continue
        stats = []
        for h in (head, head + 2):
            stats += as_rows(peak, h) + as_rows(total, h)
        empty = jnp.zeros((STAT_ROWS - len(stats), HEAD_SIZE), jnp.bfloat16)
        stats = jnp.concatenate(stats + [empty], axis=0)
        for side in range(2):
            to = head + 2 * side
            out[to, :HEAD_SIZE, :] = jnp.concatenate(
                [
                    weighted[h * HEAD_SIZE + i : h * HEAD_SIZE + i + 16]
                    for h in (head, head + 2)
                    for i in range(16 * side, HEAD_SIZE, 32)
                ],
                axis=0,
            ).astype(jnp.bfloat16)
            out[to, HEAD_SIZE:, :] = stats


def combine_kernel(partials, own, pair):
    is_high = lax.rem(lax.axis_index("tp"), 4) >= 2
    half = HEAD_SIZE // 2
    row = lax.broadcasted_iota(jnp.int32, (half, HEAD_SIZE), 0)
    lane = lax.broadcasted_iota(jnp.int32, (half, HEAD_SIZE), 1)
    place = row + (row // 16) * 16 + jnp.where(is_high, 16, 0)
    selection = (lane == place).astype(jnp.float32)
    stats = [partials[j, HEAD_SIZE:, :].astype(jnp.float32) for j in range(GROUP)]
    results = []
    for k in range(2):
        peaks = [s[6 * k : 6 * k + 1] + s[6 * k + 1 : 6 * k + 2] + s[6 * k + 2 : 6 * k + 3] for s in stats]
        totals = [s[6 * k + 3 : 6 * k + 4] + s[6 * k + 4 : 6 * k + 5] + s[6 * k + 5 : 6 * k + 6] for s in stats]
        peak = peaks[0]
        for p in peaks[1:]:
            peak = jnp.maximum(peak, p)
        fades = [jnp.exp2((p - peak) * EXP2_SCALE) for p in peaks]
        total = fades[0] * totals[0]
        for f, t in zip(fades[1:], totals[1:]):
            total += f * t
        attended = 0.0
        for j in range(GROUP):
            column = jnp.sum(selection * (fades[j] / total), axis=1, keepdims=True)
            attended += column * partials[j, half * k : half * (k + 1), :].astype(jnp.float32)
        results.append(attended.astype(jnp.bfloat16))
    low, high = results
    own[...] = jnp.where(is_high, high, low)
    pair[...] = jnp.where(is_high, low, high)


def output_kernel(own, pair, own_weight, pair_weight, out):
    update = jnp.dot(own[...], own_weight[...], preferred_element_type=jnp.float32)
    update += jnp.dot(pair[...], pair_weight[...], preferred_element_type=jnp.float32)
    out[...] = update.astype(jnp.bfloat16).reshape(out.shape)


def final_kernel(target, parts, out):
    update = parts[0].astype(jnp.float32)
    for i in range(1, parts.shape[0]):
        update += parts[i].astype(jnp.float32)
    out[...] = (target[...].astype(jnp.float32) + update).astype(jnp.bfloat16)


def call(kernel, outs, estimate, specs, out_specs=None, scratch=(), vmem=32 * 1024 * 1024):
    return pl.pallas_call(
        kernel,
        out_shape=outs,
        in_specs=specs,
        scratch_shapes=list(scratch),
        out_specs=out_specs or jax.tree.map(lambda _: VMEM, outs),
        cost_estimate=estimate,
        compiler_params=pltpu.CompilerParams(vmem_limit_bytes=vmem),
    )


def bf16(*shape):
    return jax.ShapeDtypeStruct(shape, jnp.bfloat16)


def body(
    target,
    source,
    target_gain,
    source_gain,
    query_weight,
    key_matrix,
    value_matrix,
    query_gain,
    key_gain,
    out_weight,
):
    width = target.shape[1]
    tp = lax.axis_size("tp")
    sp = lax.axis_size("sp")
    own_rows = target.shape[0]
    block = own_rows * tp
    source_rows = source.shape[0]
    halves = [[i + h * GROUP for i in range(GROUP)] for h in range(KEY_VALUE_HEADS)]
    sides = [[i for i in range(tp) if i // 2 % 2 == e] for e in range(2)]
    along_z = [[2 * z + (z + core) % 2 for z in range(sp // 2)] for core in range(2)]
    side = math.isqrt(tp)
    opposite = [(i, (side - 1 - i // side) * side + i % side) for i in range(tp)]
    depth = width // 4

    pieces = (source_rows, 2 * HEAD_SIZE)
    own, other, target_copies, target_gain_here, query_gain_here = call(
        key_value_kernel,
        (
            pltpu.VMEM(pieces, jnp.bfloat16),
            pltpu.VMEM(pieces, jnp.bfloat16),
            pltpu.HBM((tp, own_rows, width), jnp.bfloat16),
            pltpu.VMEM((1, width), jnp.float32),
            pltpu.VMEM((1, HEAD_SIZE), jnp.float32),
        ),
        cost(2 * source_rows * width * 512, 3000000),
        [HBM] * 8,
        (VMEM, VMEM, HBM, VMEM, VMEM),
        (
            pltpu.VMEM((own_rows, width), jnp.bfloat16),
            pltpu.VMEM((source_rows, width), jnp.bfloat16),
            pltpu.VMEM((1, width), jnp.float32),
            pltpu.VMEM((KEY_VALUE_HEADS, HEAD_SIZE), jnp.float32),
            pltpu.VMEM((4, depth, 2 * HEAD_SIZE), jnp.bfloat16),
            pltpu.VMEM((4, depth, 2 * HEAD_SIZE), jnp.bfloat16),
            pltpu.SemaphoreType.DMA((6,)),
            pltpu.SemaphoreType.DMA((4, 2)),
            pltpu.SemaphoreType.DMA((tp,)),
        ),
        vmem=16 * 1024 * 1024,
    )(
        *(
            pltpu.with_memory_space_constraint(x, pltpu.HBM)
            for x in (
                target,
                source,
                source_gain.reshape(1, width),
                key_matrix,
                value_matrix,
                key_gain,
                target_gain.reshape(1, width),
                query_gain,
            )
        )
    )
    received = lax.ppermute(other, "tp", opposite)
    everyone = lax.all_to_all(target_copies, "tp", 0, 0, tiled=True)
    everyone = everyone.reshape(block, width)
    near = lax.all_gather(
        jnp.concatenate([own, received], axis=0),
        "sp",
        axis=0,
        tiled=True,
        axis_index_groups=along_z,
    )
    copies = call(
        query_kernel,
        pltpu.HBM((GROUP, block, HEAD_SIZE), jnp.bfloat16),
        cost(2 * block * width * HEAD_SIZE, 1400000),
        [VMEM] * 4,
        HBM,
        (
            pltpu.VMEM((block, HEAD_SIZE), jnp.bfloat16),
            pltpu.SemaphoreType.DMA((GROUP,)),
        ),
    )(everyone, target_gain_here, query_weight, query_gain_here)
    all_queries = lax.all_to_all(
        copies, "tp", 0, 0, tiled=True, axis_index_groups=halves
    )
    far = lax.ppermute(near, "sp", [(i, i ^ 1) for i in range(sp)])
    pair_weight = lax.ppermute(out_weight, "tp", [(i, i ^ 2) for i in range(tp)])
    keys = near.shape[0]
    work = cost(
        4 * GROUP * block * keys * HEAD_SIZE, 2500000, GROUP * block * keys
    )
    carried = pltpu.VMEM((GROUP * block, HEAD_SIZE), jnp.float32)
    state = call(near_kernel, (carried,) * 3, work, [VMEM] * 2, (VMEM,) * 3)(
        all_queries, near
    )
    partials = call(
        far_kernel, bf16(GROUP, block + STAT_ROWS, HEAD_SIZE), work, [VMEM] * 5
    )(all_queries, far, *state)
    mine = lax.all_to_all(partials, "tp", 0, 0, tiled=True, axis_index_groups=halves)
    half = bf16(block // 2, HEAD_SIZE)
    own_part, pair_part = call(
        combine_kernel, (half, half), cost(4 * GROUP * block * HEAD_SIZE, 400000), [VMEM]
    )(mine)
    update = call(
        output_kernel,
        bf16(tp // 2, own_rows, width),
        cost(2 * block * width * HEAD_SIZE, 1900000),
        [VMEM] * 4,
    )(own_part, pair_part, out_weight, pair_weight)
    parts = lax.all_to_all(update, "tp", 0, 0, tiled=True, axis_index_groups=sides)
    return call(
        final_kernel,
        bf16(own_rows, width),
        cost(tp // 2 * own_rows * width, 300000),
        [VMEM] * 2,
    )(target, parts)


def solution(mesh):
    return jax.shard_map(
        body,
        mesh=mesh,
        in_specs=(
            P(("sp", "tp"), None),
            P(("sp", "tp"), None),
            P(),
            P(),
            P(None, "tp"),
            P(),
            P(),
            P("tp", None),
            P(),
            P("tp", None),
        ),
        out_specs=P(("sp", "tp"), None),
        check_vma=False,
    )
```

```python
import math

import jax
import jax.numpy as jnp
from jax import lax
from jax.experimental import pallas as pl
from jax.experimental.pallas import tpu as pltpu
from jax.sharding import PartitionSpec as P


QUERY_HEAD_COUNT = 16
KEY_VALUE_HEADS = 2
HEAD_SIZE = 128
GROUP = QUERY_HEAD_COUNT // KEY_VALUE_HEADS
EPSILON = 1e-06
EXP2_SCALE = math.log2(math.e) / math.sqrt(HEAD_SIZE)
STAT_ROWS = 16

VMEM = pl.BlockSpec(memory_space=pltpu.VMEM)
HBM = pl.BlockSpec(memory_space=pltpu.HBM)


def cost(flops, nbytes, transcendentals=0):
    return pl.CostEstimate(
        flops=flops, bytes_accessed=nbytes, transcendentals=transcendentals
    )


def normed(values_in, gain):
    return (
        values_in
        * lax.rsqrt(jnp.mean(values_in * values_in, axis=-1, keepdims=True) + EPSILON)
        * gain
    )


def key_value_kernel(
    target,
    source,
    gain,
    key_matrix,
    value_matrix,
    key_gain,
    target_gain,
    query_gain,
    own,
    other,
    target_copies,
    target_gain_here,
    query_gain_here,
    target_here,
    source_here,
    gain_here,
    key_gain_here,
    key_part,
    value_part,
    arrived,
    matrix_arrived,
    left,
):
    depth = key_part.shape[1]
    parts = key_part.shape[0]
    inputs = [
        pltpu.make_async_copy(a, b, arrived.at[i])
        for i, (a, b) in enumerate(
            (
                (target, target_here),
                (source, source_here),
                (gain, gain_here),
                (key_gain, key_gain_here),
                (target_gain, target_gain_here),
                (query_gain, query_gain_here),
            )
        )
    ]
    matrices = [
        pltpu.make_async_copy(
            matrix.at[pl.ds(i * depth, depth), :], buffer.at[i], matrix_arrived.at[i, j]
        )
        for i in range(parts)
        for j, (matrix, buffer) in enumerate(
            ((key_matrix, key_part), (value_matrix, value_part))
        )
    ]
    outputs = [
        pltpu.make_async_copy(target_here, target_copies.at[i], left.at[i])
        for i in range(target_copies.shape[0])
    ]
    for c in inputs + matrices:
        c.start()
    inputs[0].wait()
    for c in outputs:
        c.start()
    second = lax.axis_index("tp") >= GROUP
    for c in inputs[1:]:
        c.wait()
    rows = normed(source_here[...].astype(jnp.float32), gain_here[...])
    rows = rows.astype(jnp.bfloat16)
    raw, values = 0.0, 0.0
    for i in range(parts):
        matrices[2 * i].wait()
        matrices[2 * i + 1].wait()
        part = rows[:, i * depth : (i + 1) * depth]
        raw += jnp.dot(part, key_part[i], preferred_element_type=jnp.float32)
        values += jnp.dot(part, value_part[i], preferred_element_type=jnp.float32)
    values = values.astype(jnp.bfloat16)
    heads = []
    for h in range(KEY_VALUE_HEADS):
        at = slice(h * HEAD_SIZE, (h + 1) * HEAD_SIZE)
        keys = normed(raw[:, at], key_gain_here[h : h + 1, :]).astype(jnp.bfloat16)
        heads.append(jnp.concatenate([keys, values[:, at]], axis=1))
    own[...] = jnp.where(second, heads[1], heads[0])
    other[...] = jnp.where(second, heads[0], heads[1])
    for c in outputs:
        c.wait()


def query_kernel(target, gain, weight, head_gain, copies, here, left):
    rows = normed(target[...].astype(jnp.float32), gain[...]).astype(jnp.bfloat16)
    raw = jnp.dot(rows, weight[...], preferred_element_type=jnp.float32)
    here[...] = normed(raw, head_gain[...]).astype(jnp.bfloat16)
    outputs = [
        pltpu.make_async_copy(here, copies.at[i], left.at[i]) for i in range(GROUP)
    ]
    for c in outputs:
        c.start()
    for c in outputs:
        c.wait()


def in_three(x):
    first = x.astype(jnp.bfloat16)
    rest = x - first.astype(jnp.float32)
    second = rest.astype(jnp.bfloat16)
    third = (rest - second.astype(jnp.float32)).astype(jnp.bfloat16)
    return [first, second, third]


def attention_kernel(queries, near, far, out):
    rows = GROUP * HEAD_SIZE
    at_row = lax.broadcasted_iota(jnp.int32, (HEAD_SIZE, HEAD_SIZE), 0)
    at_lane = lax.broadcasted_iota(jnp.int32, (HEAD_SIZE, HEAD_SIZE), 1)
    eye = (at_row == at_lane).astype(jnp.float32)
    q = queries[...].reshape(rows, HEAD_SIZE)
    peak = None
    for kv in (near, far):
        scores = lax.dot_general(
            q,
            kv[:, :HEAD_SIZE],
            (((1,), (1,)), ((), ())),
            preferred_element_type=jnp.float32,
        )
        highest = jnp.max(scores, axis=-1, keepdims=True)
        before, peak = peak, highest if peak is None else jnp.maximum(peak, highest)
        weights = jnp.exp2((scores - peak) * EXP2_SCALE)
        share = jnp.sum(weights, axis=-1, keepdims=True)
        part = jnp.dot(
            weights.astype(jnp.bfloat16),
            kv[:, HEAD_SIZE:],
            preferred_element_type=jnp.float32,
        )
        if before is None:
            total, weighted = share, part
        else:
            fade = jnp.exp2((before - peak) * EXP2_SCALE)
            total, weighted = total * fade + share, weighted * fade + part

    def as_rows(column, head):
        at = slice(head * HEAD_SIZE, (head + 1) * HEAD_SIZE)
        return in_three(jnp.sum(eye * column[at], axis=0, keepdims=True))

    for head in range(GROUP):
        if head % 4 >= 2:
            continue
        opposite = head + 3 - 2 * (head % 4)
        stats = []
        for h in (head, opposite):
            stats += as_rows(peak, h) + as_rows(total, h)
        empty = jnp.zeros((STAT_ROWS - len(stats), HEAD_SIZE), jnp.bfloat16)
        stats = jnp.concatenate(stats + [empty], axis=0)
        for side in range(2):
            to = opposite if side else head
            out[to, :HEAD_SIZE, :] = jnp.concatenate(
                [
                    weighted[h * HEAD_SIZE + i : h * HEAD_SIZE + i + 16]
                    for h in (head, opposite)
                    for i in range(16 * side, HEAD_SIZE, 32)
                ],
                axis=0,
            ).astype(jnp.bfloat16)
            out[to, HEAD_SIZE:, :] = stats


def combine_kernel(partials, own, pair):
    is_high = lax.rem(lax.axis_index("tp"), 4) >= 2
    half = HEAD_SIZE // 2
    row = lax.broadcasted_iota(jnp.int32, (half, HEAD_SIZE), 0)
    lane = lax.broadcasted_iota(jnp.int32, (half, HEAD_SIZE), 1)
    place = row + (row // 16) * 16 + jnp.where(is_high, 16, 0)
    selection = (lane == place).astype(jnp.float32)
    stats = [partials[j, HEAD_SIZE:, :].astype(jnp.float32) for j in range(GROUP)]
    results = []
    for k in range(2):
        peaks = [s[6 * k : 6 * k + 1] + s[6 * k + 1 : 6 * k + 2] + s[6 * k + 2 : 6 * k + 3] for s in stats]
        totals = [s[6 * k + 3 : 6 * k + 4] + s[6 * k + 4 : 6 * k + 5] + s[6 * k + 5 : 6 * k + 6] for s in stats]
        peak = peaks[0]
        for p in peaks[1:]:
            peak = jnp.maximum(peak, p)
        fades = [jnp.exp2((p - peak) * EXP2_SCALE) for p in peaks]
        total = fades[0] * totals[0]
        for f, t in zip(fades[1:], totals[1:]):
            total += f * t
        attended = 0.0
        for j in range(GROUP):
            column = jnp.sum(selection * (fades[j] / total), axis=1, keepdims=True)
            attended += column * partials[j, half * k : half * (k + 1), :].astype(jnp.float32)
        results.append(attended.astype(jnp.bfloat16))
    low, high = results
    own[...] = jnp.where(is_high, high, low)
    pair[...] = jnp.where(is_high, low, high)


def output_kernel(own, pair, own_weight, pair_weight, out):
    update = jnp.dot(own[...], own_weight[...], preferred_element_type=jnp.float32)
    update += jnp.dot(pair[...], pair_weight[...], preferred_element_type=jnp.float32)
    out[...] = update.astype(jnp.bfloat16).reshape(out.shape)


def final_kernel(target, parts, out):
    update = parts[0].astype(jnp.float32)
    for i in range(1, parts.shape[0]):
        update += parts[i].astype(jnp.float32)
    out[...] = (target[...].astype(jnp.float32) + update).astype(jnp.bfloat16)


def call(kernel, outs, estimate, specs, out_specs=None, scratch=(), vmem=48 * 1024 * 1024):
    return pl.pallas_call(
        kernel,
        out_shape=outs,
        in_specs=specs,
        scratch_shapes=list(scratch),
        out_specs=out_specs or jax.tree.map(lambda _: VMEM, outs),
        cost_estimate=estimate,
        compiler_params=pltpu.CompilerParams(vmem_limit_bytes=vmem),
    )


def bf16(*shape):
    return jax.ShapeDtypeStruct(shape, jnp.bfloat16)


def body(
    target,
    source,
    target_gain,
    source_gain,
    query_weight,
    key_matrix,
    value_matrix,
    query_gain,
    key_gain,
    out_weight,
):
    width = target.shape[1]
    tp = lax.axis_size("tp")
    sp = lax.axis_size("sp")
    own_rows = target.shape[0]
    block = own_rows * tp
    source_rows = source.shape[0]
    halves = [[i + h * GROUP for i in range(GROUP)] for h in range(KEY_VALUE_HEADS)]
    sides = [[i for i in range(tp) if i // 2 % 2 == e] for e in range(2)]
    along_z = [[2 * z + (z + core) % 2 for z in range(sp // 2)] for core in range(2)]
    side = math.isqrt(tp)
    opposite = [(i, (side - 1 - i // side) * side + i % side) for i in range(tp)]
    depth = width // 4

    pieces = (source_rows, 2 * HEAD_SIZE)
    own, other, target_copies, target_gain_here, query_gain_here = call(
        key_value_kernel,
        (
            pltpu.VMEM(pieces, jnp.bfloat16),
            pltpu.VMEM(pieces, jnp.bfloat16),
            pltpu.HBM((tp, own_rows, width), jnp.bfloat16),
            pltpu.VMEM((1, width), jnp.float32),
            pltpu.VMEM((1, HEAD_SIZE), jnp.float32),
        ),
        cost(2 * source_rows * width * 512, 3000000),
        [HBM] * 8,
        (VMEM, VMEM, HBM, VMEM, VMEM),
        (
            pltpu.VMEM((own_rows, width), jnp.bfloat16),
            pltpu.VMEM((source_rows, width), jnp.bfloat16),
            pltpu.VMEM((1, width), jnp.float32),
            pltpu.VMEM((KEY_VALUE_HEADS, HEAD_SIZE), jnp.float32),
            pltpu.VMEM((4, depth, 2 * HEAD_SIZE), jnp.bfloat16),
            pltpu.VMEM((4, depth, 2 * HEAD_SIZE), jnp.bfloat16),
            pltpu.SemaphoreType.DMA((6,)),
            pltpu.SemaphoreType.DMA((4, 2)),
            pltpu.SemaphoreType.DMA((tp,)),
        ),
        vmem=16 * 1024 * 1024,
    )(
        *(
            pltpu.with_memory_space_constraint(x, pltpu.HBM)
            for x in (
                target,
                source,
                source_gain.reshape(1, width),
                key_matrix,
                value_matrix,
                key_gain,
                target_gain.reshape(1, width),
                query_gain,
            )
        )
    )
    received = lax.ppermute(other, "tp", opposite)
    everyone = lax.all_to_all(target_copies, "tp", 0, 0, tiled=True)
    everyone = everyone.reshape(block, width)
    near = lax.all_gather(
        jnp.concatenate([own, received], axis=0),
        "sp",
        axis=0,
        tiled=True,
        axis_index_groups=along_z,
    )
    copies = call(
        query_kernel,
        pltpu.HBM((GROUP, block, HEAD_SIZE), jnp.bfloat16),
        cost(2 * block * width * HEAD_SIZE, 1400000),
        [VMEM] * 4,
        HBM,
        (
            pltpu.VMEM((block, HEAD_SIZE), jnp.bfloat16),
            pltpu.SemaphoreType.DMA((GROUP,)),
        ),
    )(everyone, target_gain_here, query_weight, query_gain_here)
    all_queries = lax.all_to_all(
        copies, "tp", 0, 0, tiled=True, axis_index_groups=halves
    )
    far = lax.ppermute(near, "sp", [(i, i ^ 1) for i in range(sp)])
    pair_weight = lax.ppermute(out_weight, "tp", [(i, i ^ 3) for i in range(tp)])
    keys = 2 * near.shape[0]
    partials = call(
        attention_kernel,
        bf16(GROUP, block + STAT_ROWS, HEAD_SIZE),
        cost(4 * GROUP * block * keys * HEAD_SIZE, 2500000, GROUP * block * keys),
        [VMEM] * 3,
    )(all_queries, near, far)
    mine = lax.all_to_all(partials, "tp", 0, 0, tiled=True, axis_index_groups=halves)
    half = bf16(block // 2, HEAD_SIZE)
    own_part, pair_part = call(
        combine_kernel, (half, half), cost(4 * GROUP * block * HEAD_SIZE, 400000), [VMEM]
    )(mine)
    update = call(
        output_kernel,
        bf16(tp // 2, own_rows, width),
        cost(2 * block * width * HEAD_SIZE, 1900000),
        [VMEM] * 4,
    )(own_part, pair_part, out_weight, pair_weight)
    parts = lax.all_to_all(update, "tp", 0, 0, tiled=True, axis_index_groups=sides)
    return call(
        final_kernel,
        bf16(own_rows, width),
        cost(tp // 2 * own_rows * width, 300000),
        [VMEM] * 2,
    )(target, parts)


def solution(mesh):
    return jax.shard_map(
        body,
        mesh=mesh,
        in_specs=(
            P(("sp", "tp"), None),
            P(("sp", "tp"), None),
            P(),
            P(),
            P(None, "tp"),
            P(),
            P(),
            P("tp", None),
            P(),
            P("tp", None),
        ),
        out_specs=P(("sp", "tp"), None),
        check_vma=False,
    )
```
